256 devices in a mesh: sp: 64 (over z, y, core), tp: 4 (over x).
Axes of the slice: x: 4, y: 4, z: 8, core: 2. Of those that a mesh axis runs over, the one named last changes fastest.
Arguments:
- expert_in: bfloat16 [8192, 2048], P('sp'), may hold values from -6 to 6
- out_cot: bfloat16 [8192, 2048], P('sp'), may hold values from -16 to 16
- route_ids: int32 [8192, 2], P('sp'), may hold values from 0 to 63, all different within a row; in each aligned block of 128 rows (0 to 127, 128 to 255, ...) at most 8 rows name the same one
- route_weights: float32 [8192, 2], P('sp'), may hold values from 0.1 to 1
- w_gate: bfloat16 [64, 2048, 1024], P('sp', None, 'tp'), may hold values from -0.125 to 0.125
- w_up: bfloat16 [64, 2048, 1024], P('sp', None, 'tp'), may hold values from -0.125 to 0.125
- w_down: bfloat16 [64, 1024, 2048], P('sp', 'tp'), may hold values from -0.1875 to 0.1875
- w_out: bfloat16 [2048, 1024], P(None, 'tp'), may hold values from -0.1875 to 0.1875
- mixed_heads: bfloat16 [8192, 1024], P('sp', 'tp'), may hold values from -6 to 6
- queries: bfloat16 [8192, 512], P('sp', 'tp'), may hold values from -0.5 to 0.5
- keys: bfloat16 [8192, 512], P('sp', 'tp'), may hold values from -0.3125 to 0.3125
- values: bfloat16 [8192, 1024], P('sp', 'tp'), may hold values from -6 to 6
- log_decay: float32 [8192, 512], P('sp', 'tp'), may hold values from -0.3 to 0
Outputs:
- grad_gate: float32 [64, 2048, 1024], P('sp', None, 'tp')
- grad_up: float32 [64, 2048, 1024], P('sp', None, 'tp')
- grad_down: float32 [64, 1024, 2048], P('sp', 'tp')
- grad_out_proj: float32 [2048, 1024], P('sp', 'tp')
- grad_queries: bfloat16 [8192, 512], P('sp', 'tp')
- grad_keys: bfloat16 [8192, 512], P('sp', 'tp')
- grad_values: bfloat16 [8192, 1024], P('sp', 'tp')
- grad_decay: float32 [8192, 512], P('sp', 'tp')
The draws below stay inside these ranges and needn't reach their ends.
Inputs may be any that keep to these rules, and one draw needn't show every extreme that they name: `route_ids`: in the rows of one device no expert is named more than 8 times, a bound that some block reaches.
All inputs are finite; a program needn't handle non-finite values.
Results may differ from the reference program's by a relative error of at most 0.015.
Values may be sent and summed in bfloat16 or wider, within the bound.
No kernel may reach another device: no remote copies, remote signals or barrier semaphores. Data moves between devices by JAX's collectives and lax.ppermute only.
A program may use at most 128 MiB of HBM per device.

```python
import math
import jax
import jax.numpy as jnp
import numpy as np
from jax import lax

D = 2048
FF = 1024
HEADS = 4
DK = 128
DV = 256
BLK = 128
TOP_K = 2
TOK_DEV = 128
EXPERTS = 64
CAP = 8
TOKENS = 8192
N_SP = 64
N_TP = 4


def draw_log_decay(key, part):
    channels = HEADS * DK
    keys_list = jax.random.split(key, 5)
    slow_share = 0.5
    is_slow = jax.random.uniform(keys_list[0], (channels,), jnp.float32) < slow_share
    slow_rate = jax.random.uniform(keys_list[1], (channels,), jnp.float32, 0.1, 0.5) / TOKENS
    fast_rate = jax.random.uniform(keys_list[2], (channels,), jnp.float32, 0.05, 0.1)
    decay_rate = jnp.where(is_slow, slow_rate, fast_rate)
    span_factor = jnp.exp(jax.random.uniform(keys_list[3], (TOKENS // BLK, 1, 1), jnp.float32, -math.log(2.0), math.log(2.0)))
    roughness = jax.random.uniform(keys_list[4], (TOKENS // BLK, BLK, channels), jnp.float32, 0.5, 1.5)
    return (-(decay_rate * span_factor * roughness)).reshape(TOKENS, channels)


def with_spikes(drawn, key, source, target, parts, factor):
    owner, partner = [(jnp.arange(drawn.shape[dim]) // (drawn.shape[dim] // parts)).reshape([-1 if axis == dim else 1 for axis in range(drawn.ndim)]) for dim in (source, target)]
    chosen = jax.random.permutation(key, parts)[partner]
    strong = (owner == chosen) | (owner == (partner + parts // 2) % parts)
    return jnp.where(strong, factor * drawn, drawn)


def block_scale(own_key, dims, cuts, least, largest):
    level = 1.0
    for dim, parts in cuts:
        steps = jax.random.uniform(jax.random.fold_in(jax.random.fold_in(own_key, 6), dim), (parts,), jnp.float32, least / len(cuts), largest / len(cuts))
        level = level * jnp.repeat(jnp.exp(steps), dims[dim] // parts).reshape((-1,) + (1,) * (len(dims) - 1 - dim))
    return level


def shared_out(key, own, number, rows, count, top, most, lean):
    sequence = jax.random.permutation(key, count)
    heavy_load, ordinary = portions_of(count, rows * top, most, lean, True), portions_of(count, rows * top, most, lean, False)
    places = jnp.arange(count)

    def named(lengths, turn):
        used = int((lengths > 0).sum())
        fixed = max(1, used // 4)
        shifted = fixed + (places - fixed + turn * (used - fixed)) % max(1, count - fixed)
        return jnp.zeros((count,), jnp.int32).at[sequence[jnp.where(places < fixed, places, shifted)]].set(jnp.asarray(lengths, jnp.int32))

    lengths = jnp.where(number % 4 == 0, named(heavy_load, number // 4), named(ordinary, number - number // 4 - 1))
    mixed = jax.random.permutation(jax.random.fold_in(own, 3), count)
    source_of, sink = mixed[0:count // 2 * 2:2], mixed[1:count // 2 * 2:2]
    slack = jnp.minimum(lengths[source_of] - 1, most - lengths[sink]) // 2
    slack = jnp.where((source_of == sequence[0]) | (sink == sequence[0]) | (lengths[sink] == 0), 0, jnp.maximum(slack, 0))
    shifted = jax.random.randint(jax.random.fold_in(own, 4), (count // 2,), 0, 1 << 20) % (slack + 1)
    lengths = lengths.at[source_of].add(-shifted).at[sink].add(shifted)
    labels = jnp.searchsorted(jnp.cumsum(lengths), jnp.arange(rows * top), side="right").astype(jnp.int32)
    table = labels.reshape(top, rows).T
    table = table[jax.random.permutation(jax.random.fold_in(own, 1), rows)]
    turn = jax.random.randint(jax.random.fold_in(own, 2), (rows, 1), 0, top)
    return jnp.take_along_axis(table, (jnp.arange(top)[None, :] + turn) % top, axis=1)


def portions_of(amount, total, bound, skew, full):
    portions = [(1 << 20) // math.isqrt(grade ** skew) + 1 for grade in range(1, amount + 1)]
    largest = bound if full else min(bound, max(-(-total // amount), total * portions[0] // sum(portions)))
    least = 1 if total - largest >= amount - 1 else 0
    given, rest = [largest] + [least] * (amount - 1), total - largest - least * (amount - 1)
    while rest > 0:
        free = [i for i in range(1, amount) if given[i] < largest] or [i for i in range(1, amount) if given[i] < bound]
        pool, left = sum([portions[i] for i in free]), rest
        for i in free:
            more = min(bound - given[i], max(1, left * portions[i] // pool), rest)
            given[i] = given[i] + more
            rest = rest - more
    return np.array(given)


def normal_values(own_key, shape, deviation, reach, pieces=(), kind=jnp.bfloat16):
    entries = jax.random.normal(own_key, shape, jnp.float32) * deviation
    if len(pieces) > 0:
        entries = block_scale(own_key, shape, pieces, -0.22, 0.18) * entries
    return jnp.clip(entries, min=-reach, max=reach).astype(kind)


def gaussian_with(rng, extent, width, bound, pieces, heavy, kind=jnp.bfloat16):
    result = width * jax.random.normal(rng, extent, jnp.float32)
    if pieces:
        result = result * block_scale(rng, extent, pieces, -0.22, 0.18)
    return jnp.clip(with_spikes(result, jax.random.fold_in(rng, 3), *heavy), -bound, bound).astype(kind)


def setup_inputs(seed: int = 0) -> dict:
    arg_keys = jax.random.split(jax.random.key(seed), 14)
    expert_in = normal_values(arg_keys[0], (TOKENS, D), 1.0, 6.0, ((0, 64),))
    out_cot = gaussian_with(arg_keys[1], (TOKENS, D), 1.0, 16.0, ((0, 64),), (0, 1, 64, 4.0))
    route_ids_keys = jax.random.split(jax.random.fold_in(arg_keys[2], 1), TOKENS // TOK_DEV)
    route_ids_turns = jax.random.permutation(jax.random.fold_in(arg_keys[2], 3), TOKENS // TOK_DEV)
    route_ids = jax.vmap(lambda own, number: shared_out(jax.random.fold_in(arg_keys[2], 2), own, number, TOK_DEV, EXPERTS, TOP_K, CAP, 1))(route_ids_keys, route_ids_turns).reshape((TOKENS, TOP_K))
    route_weights = jnp.clip(0.1 + 0.9 * jax.random.uniform(arg_keys[3], (TOKENS, TOP_K), jnp.float32) ** block_scale(arg_keys[3], (TOKENS, TOP_K), ((0, 64),), -0.2, 0.2), 0.1, 1.0)
    w_gate = normal_values(arg_keys[4], (EXPERTS, D, FF), D ** -0.5, 0.125, ((0, 64), (2, 4)))
    w_up = normal_values(arg_keys[5], (EXPERTS, D, FF), D ** -0.5, 0.125, ((0, 64), (2, 4)))
    w_down = normal_values(arg_keys[6], (EXPERTS, FF, D), FF ** -0.5, 0.1875, ((0, 64), (1, 4)))
    w_out = normal_values(arg_keys[7], (D, HEADS * DV), (HEADS * DV) ** -0.5, 0.1875, ((1, 4),))
    mixed_heads = normal_values(arg_keys[8], (TOKENS, HEADS * DV), 1.0, 6.0, ((0, 64), (1, 4)))
    queries = normal_values(arg_keys[9], (TOKENS, HEADS * DK), 0.09, 0.5, ((0, 64), (1, 4)))
    keys = normal_values(arg_keys[10], (TOKENS, HEADS * DK), 0.05, 0.3125, ((0, 64), (1, 4)))
    values = normal_values(arg_keys[11], (TOKENS, HEADS * DV), 1.0, 6.0, ((0, 64), (1, 4)))
    log_decay = draw_log_decay(jax.random.fold_in(arg_keys[13], 71), 0)
    return dict(expert_in=expert_in, out_cot=out_cot, route_ids=route_ids, route_weights=route_weights, w_gate=w_gate, w_up=w_up, w_down=w_down, w_out=w_out, mixed_heads=mixed_heads, queries=queries, keys=keys, values=values, log_decay=log_decay)


exact_mode = lax.Precision.HIGHEST

def block_forward(query_blocks, key_blocks, value_blocks, decay_blocks, state_start):
    block_len = query_blocks.shape[1]
    cumulative = jnp.cumsum(decay_blocks, axis=1)
    block_sum = cumulative[:, -1]
    query_decayed = query_blocks * jnp.exp(cumulative)
    key_grown = key_blocks * jnp.exp(-cumulative)
    key_to_end = key_blocks * jnp.exp(block_sum[:, None] - cumulative)
    causal = jnp.tril(jnp.ones((block_len, block_len), dtype=bool))
    scores = jnp.einsum('nchd,nshd->nhcs', query_decayed, key_grown, precision=exact_mode)
    scores = jnp.where(causal, scores, 0.0)
    intra_out = jnp.einsum('nhcs,nshe->nche', scores, value_blocks, precision=exact_mode)

    def advance(state_now, block):
        query_part, key_part, value_part, sum_part = block
        carried = jnp.einsum('chd,hde->che', query_part, state_now, precision=exact_mode)
        state_now = state_now * jnp.exp(sum_part)[..., None] + jnp.einsum('chd,che->hde', key_part, value_part, precision=exact_mode)
        return (state_now, carried)
    final_state, carried_out = lax.scan(advance, state_start, (query_decayed, key_to_end, value_blocks, block_sum))
    return (intra_out + carried_out, final_state)

def slot_table(route_ids):
    flat_ids = route_ids.reshape(N_SP, TOK_DEV * TOP_K)
    onehot = (flat_ids[..., None] == jnp.arange(EXPERTS, dtype=jnp.int32)).astype(jnp.int32)
    slot_rank = lax.optimization_barrier(jnp.sum((jnp.cumsum(onehot, axis=1) - 1) * onehot, axis=2)).astype(jnp.int32)
    source = jnp.arange(N_SP, dtype=jnp.int32)[:, None]
    slot_index = (flat_ids * (N_SP * CAP) + source * CAP + slot_rank).astype(jnp.int32)
    assign = jnp.arange(TOKENS * TOP_K, dtype=jnp.int32)
    table = jnp.full((EXPERTS * N_SP * CAP,), TOKENS * TOP_K, jnp.int32).at[slot_index.reshape(-1)].set(assign)
    return table.reshape(EXPERTS, N_SP * CAP)

def reference(expert_in, out_cot, route_ids, route_weights, w_gate, w_up, w_down, w_out, mixed_heads, queries, keys, values, log_decay):
    table = slot_table(route_ids)
    flat_weights = route_weights.reshape(-1)

    def per_expert(accum, pack):
        owners, gate_w, up_w, down_w = pack
        is_live = owners < TOKENS * TOP_K
        owner_safe = jnp.where(is_live, owners, 0)
        owner_token = owner_safe // TOP_K
        x_rows = jnp.where(is_live[:, None], expert_in[owner_token], jnp.zeros((), jnp.bfloat16))
        slot_weight = jnp.where(is_live, flat_weights[owner_safe], 0.0)
        dy_rows = (slot_weight[:, None] * out_cot[owner_token].astype(jnp.float32)).astype(jnp.bfloat16)
        gate_pre = jnp.dot(x_rows, gate_w, preferred_element_type=jnp.float32)
        up_pre = jnp.dot(x_rows, up_w, preferred_element_type=jnp.float32)
        sigmoid_gate = jax.nn.sigmoid(gate_pre)
        hidden = (gate_pre * sigmoid_gate * up_pre).astype(jnp.bfloat16)
        hidden_cot = jnp.dot(dy_rows, down_w.T, preferred_element_type=jnp.float32)
        grad_down = jnp.dot(hidden.T, dy_rows, preferred_element_type=jnp.float32)
        gate_cot = (hidden_cot * up_pre * sigmoid_gate * (1.0 + gate_pre * (1.0 - sigmoid_gate))).astype(jnp.bfloat16)
        up_cot = (hidden_cot * gate_pre * sigmoid_gate).astype(jnp.bfloat16)
        grad_gate = jnp.dot(x_rows.T, gate_cot, preferred_element_type=jnp.float32)
        grad_up = jnp.dot(x_rows.T, up_cot, preferred_element_type=jnp.float32)
        part = FF // N_TP
        rows_count = owners.shape[0]
        partial_value = jnp.einsum('snf,dnf->nsd', gate_cot.astype(jnp.float32).reshape(rows_count, N_TP, part), gate_w.astype(jnp.float32).reshape(D, N_TP, part))
        partial_value = partial_value + jnp.einsum('snf,dnf->nsd', up_cot.astype(jnp.float32).reshape(rows_count, N_TP, part), up_w.astype(jnp.float32).reshape(D, N_TP, part))
        input_cot = lax.optimization_barrier(jnp.sum(partial_value.astype(jnp.bfloat16).astype(jnp.float32), axis=0)).astype(jnp.bfloat16)
        accum = accum.at[owner_token].add(jnp.where(is_live[:, None], input_cot.astype(jnp.float32), 0.0))
        return (accum, (grad_gate, grad_up, grad_down))
    accum = jnp.zeros((TOKENS, D), jnp.float32)
    accum, (grad_gate, grad_up, grad_down) = lax.scan(per_expert, accum, (table, w_gate, w_up, w_down))
    mid_cot = (out_cot.astype(jnp.float32) + accum).astype(jnp.bfloat16)
    grad_out_proj = jnp.dot(mid_cot.T, mixed_heads, preferred_element_type=jnp.float32)
    head_cot = jnp.dot(mid_cot, w_out, preferred_element_type=jnp.float32)

    def mechanism(query_in, key_in, value_in, decay_in):
        blocks = TOKENS // BLK
        out, _ = block_forward(query_in.astype(jnp.float32).reshape(blocks, BLK, HEADS, DK), key_in.astype(jnp.float32).reshape(blocks, BLK, HEADS, DK), value_in.astype(jnp.float32).reshape(blocks, BLK, HEADS, DV), decay_in.reshape(blocks, BLK, HEADS, DK), jnp.zeros((HEADS, DK, DV), jnp.float32))
        return out.reshape(TOKENS, HEADS * DV)
    _, pull_back = jax.vjp(mechanism, queries, keys, values, log_decay)
    grad_queries, grad_keys, grad_values, grad_decay = pull_back(head_cot)
    return (grad_gate, grad_up, grad_down, grad_out_proj, grad_queries, grad_keys, grad_values, grad_decay)
```

```python
import functools

import jax
import jax.numpy as jnp
from jax import lax
from jax.experimental import pallas as pl
from jax.experimental.pallas import tpu as pltpu
from jax.sharding import PartitionSpec as P

BF = jnp.bfloat16
F32 = jnp.float32
HI = lax.Precision.HIGHEST

TOK = 128
EXPERTS = 64
CAP = 8
SLOTS = EXPERTS * CAP
WIDTH = 2048
QUART = 512
FF = 256
DK = 128
DV = 256
LANES = 128
HALF = 64


def dot(a, b, ca, cb, precision=None):
    return lax.dot_general(
        a, b, (((ca,), (cb,)), ((), ())), preferred_element_type=F32, precision=precision
    )


def iota(shape, dim):
    return lax.broadcasted_iota(jnp.int32, shape, dim)


def rounded(x):
    return x.astype(BF).astype(F32)


def lower_lanes(shape):
    return iota(shape, len(shape) - 1) < HALF


def call(kernel, out_shape, args, *, index=None, in_specs=None, out_specs=None, flops=0):
    nbytes = sum(a.size * a.dtype.itemsize for a in args)
    outs = jax.tree.leaves(out_shape)
    nbytes += sum(o.size * o.dtype.itemsize for o in outs)

    def whole(a):
        rank = len(a.shape)
        return pl.BlockSpec(a.shape, lambda i, q: (0,) * rank)

    specs = [whole(a) if s is None else s for a, s in zip(args, in_specs or [None] * len(args))]
    out_blocks = jax.tree.map(whole, out_shape)
    return pl.pallas_call(
        kernel,
        out_shape=out_shape,
        grid_spec=pltpu.PrefetchScalarGridSpec(
            num_scalar_prefetch=1, grid=(1,), in_specs=specs, out_specs=out_blocks
        ),
        compiler_params=pltpu.CompilerParams(vmem_limit_bytes=24 * 2**20),
        cost_estimate=pl.CostEstimate(
            flops=int(flops), bytes_accessed=int(nbytes), transcendentals=0
        ),
    )(index, *args)


def sds(shape, dtype):
    return jax.ShapeDtypeStruct(shape, dtype)


def quarter_rows(q):
    return pl.ds(pl.multiple_of(q * QUART, QUART), QUART)


def cumulative_sum(g):
    lower = (iota((TOK, TOK), 0) >= iota((TOK, TOK), 1)).astype(F32)
    return dot(lower, g, 1, 0, HI)


def tiles_of(state, fill=None):
    out = []
    for b in range(4):
        t = state[:, LANES * (b // 2) : LANES * (b // 2 + 1)]
        r = pltpu.roll(t, HALF, 1)
        low, up = (t, r) if b % 2 == 0 else (r, t)
        upper = fill if fill is not None else up - rounded(up)
        tile = jnp.where(lower_lanes(t.shape), rounded(low), upper)
        out.append(tile.reshape(16, 8, LANES))
    return jnp.concatenate(out, axis=1).reshape(SLOTS, LANES)


def state_of(tiles):
    both = tiles + pltpu.roll(tiles, HALF, 1)
    t = both.reshape(16, 32, LANES)
    part = [t[:, 8 * b : 8 * b + 8, :].reshape(DK, LANES) for b in range(4)]
    low = lower_lanes((DK, LANES))
    return jnp.concatenate(
        [jnp.where(low, part[0], part[1]), jnp.where(low, part[2], part[3])], axis=1
    )


def prep_kernel(q_ref, ids_ref, w_ref, x_ref, oc_ref, k_ref, v_ref, g_ref, pay_ref, pick_ref):
    expert = iota((EXPERTS, TOK), 0)
    id0, id1 = ids_ref[0:1, :], ids_ref[1:2, :]
    hit0, hit1 = expert == id0, expert == id1
    named = (hit0.astype(F32) + hit1.astype(F32)).astype(BF)
    before = (iota((TOK, TOK), 0) < iota((TOK, TOK), 1)).astype(F32).astype(BF)
    count = dot(named, before, 1, 0)
    rank0 = jnp.sum(jnp.where(hit0, count, 0.0), axis=0, keepdims=True)
    rank1 = jnp.sum(jnp.where(hit1, count, 0.0), axis=0, keepdims=True)
    slot0 = id0 * CAP + rank0.astype(jnp.int32)
    slot1 = id1 * CAP + rank1.astype(jnp.int32)
    slot = iota((SLOTS, TOK), 0)
    at0, at1 = slot == slot0, slot == slot1
    pick = (at0.astype(F32) + at1.astype(F32)).astype(BF)
    pick_ref[...] = pick
    weight = jnp.sum(
        jnp.where(at0, w_ref[0:1, :], 0.0) + jnp.where(at1, w_ref[1:2, :], 0.0),
        axis=1,
        keepdims=True,
    )
    pay_ref[:, :QUART] = dot(pick, x_ref[...], 1, 0).astype(BF)
    pay_ref[:, QUART : 2 * QUART] = (dot(pick, oc_ref[...], 1, 0) * weight).astype(BF)
    g = g_ref[...]
    cum = cumulative_sum(g)
    to_end = k_ref[...].astype(F32) * jnp.exp(cum[TOK - 1 : TOK, :] - cum)
    state = dot(to_end.T, v_ref[...].astype(F32), 1, 0, HI)
    factor = jnp.exp(jnp.sum(g.T, axis=1, keepdims=True))
    high = rounded(factor)
    lane = iota((DK, LANES), 1)
    fill = jnp.where(lane < 96, high, factor - high)
    pay_ref[:, 2 * QUART :] = tiles_of(state, fill).astype(BF)


def prefix_kernel(q_ref, in_ref, out_ref, factor_ref, work_ref):
    tiles = in_ref[...].astype(F32)
    work_ref[...] = tiles
    factor_ref[...] = jnp.broadcast_to(tiles[:, 64:65] + tiles[:, 96:97], tiles.shape)
    carry = jnp.zeros((8, LANES), F32)
    for s in range(EXPERTS):
        rows = slice(8 * s, 8 * s + 8)
        now = work_ref[rows, :]
        work_ref[rows, :] = carry
        carry = carry * factor_ref[rows, :] + now
    pre = work_ref[...]
    low = rounded(pre)
    rest = pltpu.roll(pre - low, HALF, 1)
    out_ref[...] = jnp.where(lower_lanes(pre.shape), low, rest).astype(BF)


def suffix_kernel(q_ref, in_ref, factor_ref, out_ref, work_ref):
    tiles = in_ref[...].astype(F32)
    work_ref[...] = tiles + pltpu.roll(tiles, HALF, 1)
    carry = jnp.zeros((8, LANES), F32)
    for s in reversed(range(EXPERTS)):
        rows = slice(8 * s, 8 * s + 8)
        now = work_ref[rows, :]
        work_ref[rows, :] = carry
        carry = carry * factor_ref[rows, :] + now
    suf = work_ref[...]
    low = rounded(suf)
    out_ref[...] = jnp.where(lower_lanes(suf.shape), low, suf - low).astype(BF)


def near_kernel(q_ref, own_ref, a_ref, b_ref, wg_ref, wu_ref, wd_ref, g_ref, u_ref, h_ref):
    g = u = h = None
    for n, ref in enumerate((own_ref, a_ref, b_ref)):
        rows = quarter_rows(q_ref[n])
        x, dy = ref[:, :QUART], ref[:, QUART : 2 * QUART]
        g1 = dot(x, wg_ref[rows, :], 1, 0)
        u1 = dot(x, wu_ref[rows, :], 1, 0)
        h1 = dot(dy, wd_ref[:, rows], 1, 1)
        g, u, h = (g1, u1, h1) if g is None else (g + g1, u + u1, h + h1)
    g_ref[...] = g
    u_ref[...] = u
    h_ref[...] = h


def far_kernel(
    q_ref, g_ref, u_ref, h_ref, c_ref, d_ref, wg_ref, wu_ref, wd_ref,
    far_ref, right_ref, left_ref, own_ref, hid_ref, gu_ref,
):
    rows = quarter_rows(q_ref[3])
    x = jnp.concatenate([c_ref[:, :QUART], d_ref[:, :QUART]], axis=0)
    dy = jnp.concatenate([c_ref[:, QUART:], d_ref[:, QUART:]], axis=0)
    g = g_ref[...] + dot(x, wg_ref[rows, :], 1, 0)
    u = u_ref[...] + dot(x, wu_ref[rows, :], 1, 0)
    h = h_ref[...] + dot(dy, wd_ref[:, rows], 1, 1)
    sig = jax.nn.sigmoid(g)
    hid_ref[...] = (g * sig * u).astype(BF)
    gate_cot = (h * u * sig * (1.0 + g * (1.0 - sig))).astype(BF)
    up_cot = (h * g * sig).astype(BF)
    gu_ref[:, :FF] = gate_cot
    gu_ref[:, FF:] = up_cot
    for n, ref in ((3, far_ref), (2, right_ref), (1, left_ref), (0, own_ref)):
        rows = quarter_rows(q_ref[n])
        part = dot(gate_cot, wg_ref[rows, :], 1, 1) + dot(up_cot, wu_ref[rows, :], 1, 1)
        ref[...] = part.astype(BF)


def weight_kernel(
    q_ref, own_ref, a_ref, b_ref, c_ref, d_ref, hid_ref, gu_ref, gg_ref, gup_ref, gd_ref
):
    hid_t = hid_ref[...].T
    gu = gu_ref[...]
    for n in range(4):
        rows = quarter_rows(q_ref[n])
        if n < 3:
            ref = (own_ref, a_ref, b_ref)[n]
            x, dy = ref[:, :QUART], ref[:, QUART : 2 * QUART]
        else:
            x = jnp.concatenate([c_ref[:, :QUART], d_ref[:, :QUART]], axis=0)
            dy = jnp.concatenate([c_ref[:, QUART:], d_ref[:, QUART:]], axis=0)
        both = dot(x.T, gu, 1, 0)
        gg_ref[rows, :] = both[:, :FF]
        gup_ref[rows, :] = both[:, FF:]
        gd_ref[:, rows] = dot(hid_t, dy, 1, 0)


def sum_kernel(q_ref, p0_ref, p1_ref, p2_ref, p3_ref, st_ref, out_ref):
    total = p0_ref[...].astype(F32) + p1_ref[...].astype(F32)
    total = total + p2_ref[...].astype(F32) + p3_ref[...].astype(F32)
    out_ref[:, :QUART] = total.astype(BF)
    out_ref[:, QUART:] = st_ref[...]


def combine_kernel(q_ref, rows_ref, pick_ref, oc_ref, out_ref):
    routed = dot(pick_ref[...].T, rows_ref[...], 1, 0)
    out_ref[...] = (oc_ref[...].astype(F32) + routed).astype(BF)


def head_kernel(q_ref, m0_ref, m1_ref, m2_ref, m3_ref, w_ref, qry_ref, g_ref, h_ref, pull_ref):
    head = None
    for n, ref in enumerate((m0_ref, m1_ref, m2_ref, m3_ref)):
        part = dot(ref[...], w_ref[quarter_rows(q_ref[n]), :], 1, 0)
        head = part if head is None else head + part
    h_ref[...] = head
    decayed = qry_ref[...].astype(F32) * jnp.exp(cumulative_sum(g_ref[...]))
    pull_ref[...] = tiles_of(dot(decayed.T, head, 1, 0, HI)).astype(BF)


def out_proj_kernel(q_ref, m0_ref, m1_ref, m2_ref, m3_ref, mixed_ref, out_ref):
    mixed = mixed_ref[...]
    for n, ref in enumerate((m0_ref, m1_ref, m2_ref, m3_ref)):
        out_ref[quarter_rows(q_ref[n]), :] = dot(ref[...].T, mixed, 1, 0).astype(BF)


def attend_kernel(
    q_ref, qry_ref, k_ref, v_ref, g_ref, h_ref, st_ref, cot_ref,
    gq_ref, gk_ref, gv_ref, gg_ref,
):
    qry, k, v = qry_ref[...].astype(F32), k_ref[...].astype(F32), v_ref[...].astype(F32)
    head = h_ref[...]
    state = state_of(st_ref[...].astype(F32))
    cot = state_of(cot_ref[...].astype(F32))
    cum = cumulative_sum(g_ref[...])
    last = cum[TOK - 1 : TOK, :]
    grow, shrink, to_end = jnp.exp(cum), jnp.exp(-cum), jnp.exp(last - cum)
    q_dec, k_grown, k_end = qry * grow, k * shrink, k * to_end
    causal = iota((TOK, TOK), 0) >= iota((TOK, TOK), 1)
    score = jnp.where(causal, dot(q_dec, k_grown, 1, 1, HI), 0.0)
    d_score = jnp.where(causal, dot(head, v, 1, 1, HI), 0.0)
    d_q = dot(d_score, k_grown, 1, 0, HI) + dot(head, state, 1, 1, HI)
    d_kg = dot(d_score.T, q_dec, 1, 0, HI)
    d_ke = dot(v, cot, 1, 1, HI)
    d_v = dot(score.T, head, 1, 0, HI) + dot(k_end, cot, 1, 0, HI)
    gq_ref[...] = (d_q * grow).astype(BF)
    gk_ref[...] = (d_kg * shrink + d_ke * to_end).astype(BF)
    gv_ref[...] = d_v.astype(BF)
    end = d_ke * k_end
    d_cum = d_q * q_dec - d_kg * k_grown - end
    carried = jnp.sum((state * cot).T, axis=0, keepdims=True)
    d_last = jnp.sum(end, axis=0, keepdims=True) + jnp.exp(last) * carried
    upper = (iota((TOK, TOK), 0) <= iota((TOK, TOK), 1)).astype(F32)
    gg_ref[...] = dot(upper, d_cum, 1, 0, HI) + d_last


def per_device(
    expert_in, out_cot, route_ids, route_weights, w_gate, w_up, w_down, w_out,
    mixed_heads, queries, keys, values, log_decay,
):
    me = lax.axis_index("tp")
    order = (me + jnp.array([0, 3, 1, 2], jnp.int32)) % 4
    to_right = [(i, (i + 1) % 4) for i in range(4)]
    to_left = [(i, (i + 3) % 4) for i in range(4)]
    across = [(i, (i + 2) % 4) for i in range(4)]
    wg, wu, wd = w_gate[0], w_up[0], w_down[0]
    run = functools.partial(call, index=order)

    def exchange(rows):
        width = rows.shape[1]
        got = lax.all_to_all(rows.reshape(EXPERTS, CAP, width), "sp", 0, 0, tiled=True)
        return got.reshape(SLOTS, width)

    def quarter_block():
        return pl.BlockSpec((TOK, QUART), lambda i, q: (0, q[0]))

    def lane_tile(n):
        return pl.BlockSpec((SLOTS, LANES), lambda i, q: (0, n))

    with jax.named_scope("prep"):
        pay, pick = run(
            prep_kernel,
            (sds((SLOTS, 2 * QUART + LANES), BF), sds((SLOTS, TOK), BF)),
            (route_ids.T, route_weights.T, expert_in, out_cot, keys, values, log_decay),
            in_specs=[None, None, quarter_block(), quarter_block(), None, None, None],
            flops=4e8,
        )
    with jax.named_scope("dispatch"):
        got = exchange(pay)
        rows = got[:, : 2 * QUART]
        left = lax.ppermute(rows, "tp", to_right)
        right = lax.ppermute(rows, "tp", to_left)
        far_top = lax.ppermute(left[: SLOTS // 2], "tp", to_right)
        far_bottom = lax.ppermute(right[SLOTS // 2 :], "tp", to_left)
    with jax.named_scope("near"):
        g, u, h = run(
            near_kernel,
            (sds((SLOTS, FF), F32),) * 3,
            (got, left, right, wg, wu, wd),
            flops=1.2e9,
        )
    with jax.named_scope("far"):
        p_far, p_right, p_left, p_own, hidden, gate_up = run(
            far_kernel,
            (sds((SLOTS, QUART), BF),) * 4 + (sds((SLOTS, FF), BF), sds((SLOTS, 2 * FF), BF)),
            (g, u, h, far_top, far_bottom, wg, wu, wd),
            flops=1.5e9,
        )
    with jax.named_scope("scatter"):
        r_far = lax.ppermute(p_far, "tp", across)
        r_left = lax.ppermute(p_right, "tp", to_right)
        r_right = lax.ppermute(p_left, "tp", to_left)
    with jax.named_scope("prefix"):
        state_back, factor = pl.pallas_call(
            prefix_kernel,
            out_shape=(sds((SLOTS, LANES), BF), sds((SLOTS, LANES), F32)),
            grid_spec=pltpu.PrefetchScalarGridSpec(
                num_scalar_prefetch=1,
                grid=(1,),
                in_specs=[lane_tile(2 * QUART // LANES)],
                out_specs=(lane_tile(0), lane_tile(0)),
                scratch_shapes=[pltpu.VMEM((SLOTS, LANES), F32)],
            ),
            compiler_params=pltpu.CompilerParams(vmem_limit_bytes=8 * 2**20),
            cost_estimate=pl.CostEstimate(flops=10**8, bytes_accessed=10**6, transcendentals=0),
        )(order, got)
    with jax.named_scope("weights"):
        grad_gate, grad_up, grad_down = run(
            weight_kernel,
            (sds((WIDTH, FF), F32), sds((WIDTH, FF), F32), sds((FF, WIDTH), F32)),
            (got, left, right, far_top, far_bottom, hidden, gate_up),
            flops=1.6e9 * 4,
        )
    with jax.named_scope("back"):
        total = run(
            sum_kernel,
            sds((SLOTS, QUART + LANES), BF),
            (p_own, r_far, r_left, r_right, state_back),
            flops=1e6,
        )
        back = exchange(total)
        mid = run(
            combine_kernel,
            sds((TOK, QUART), BF),
            (back, pick, out_cot),
            in_specs=[pl.BlockSpec((SLOTS, QUART), lambda i, q: (0, 0)), None, quarter_block()],
            flops=7e7,
        )
        m_left = lax.ppermute(mid, "tp", to_right)
        m_right = lax.ppermute(mid, "tp", to_left)
        m_far = lax.ppermute(mid, "tp", across)
    with jax.named_scope("head"):
        head, pull = run(
            head_kernel,
            (sds((TOK, DV), F32), sds((SLOTS, LANES), BF)),
            (mid, m_left, m_right, m_far, w_out, queries, log_decay),
            flops=2e8,
        )
        pulled = exchange(pull)
    with jax.named_scope("out_proj"):
        part = run(
            out_proj_kernel,
            sds((WIDTH, DV), BF),
            (mid, m_left, m_right, m_far, mixed_heads),
            flops=1.4e8,
        )
        parts = lax.all_to_all(part.reshape(64, 32, DV), "sp", 0, 0, tiled=True)
        grad_out_proj = jnp.sum(parts.astype(F32), axis=0)
    with jax.named_scope("suffix"):
        cot_back = pl.pallas_call(
            suffix_kernel,
            out_shape=sds((SLOTS, LANES), BF),
            grid_spec=pltpu.PrefetchScalarGridSpec(
                num_scalar_prefetch=1,
                grid=(1,),
                in_specs=[lane_tile(0), lane_tile(0)],
                out_specs=lane_tile(0),
                scratch_shapes=[pltpu.VMEM((SLOTS, LANES), F32)],
            ),
            compiler_params=pltpu.CompilerParams(vmem_limit_bytes=8 * 2**20),
            cost_estimate=pl.CostEstimate(flops=10**8, bytes_accessed=10**6, transcendentals=0),
        )(order, pulled, factor)
        cot = exchange(cot_back)
    with jax.named_scope("attend"):
        grad_queries, grad_keys, grad_values, grad_decay = run(
            attend_kernel,
            (sds((TOK, DK), BF), sds((TOK, DK), BF), sds((TOK, DV), BF), sds((TOK, DK), F32)),
            (queries, keys, values, log_decay, head, back, cot),
            in_specs=[None] * 5 + [lane_tile(QUART // LANES), None],
            flops=6e8,
        )
    return (
        grad_gate[None],
        grad_up[None],
        grad_down[None],
        grad_out_proj,
        grad_queries,
        grad_keys,
        grad_values,
        grad_decay,
    )


def solution(mesh):
    return jax.shard_map(
        per_device,
        mesh=mesh,
        in_specs=(
            P("sp", None),
            P("sp", None),
            P("sp", None),
            P("sp", None),
            P("sp", None, "tp"),
            P("sp", None, "tp"),
            P("sp", "tp", None),
            P(None, "tp"),
            P("sp", "tp"),
            P("sp", "tp"),
            P("sp", "tp"),
            P("sp", "tp"),
            P("sp", "tp"),
        ),
        out_specs=(
            P("sp", None, "tp"),
            P("sp", None, "tp"),
            P("sp", "tp", None),
            P("sp", "tp"),
            P("sp", "tp"),
            P("sp", "tp"),
            P("sp", "tp"),
            P("sp", "tp"),
        ),
        check_vma=False,
    )
```

```python
import functools

import jax
import jax.numpy as jnp
from jax import lax
from jax.experimental import pallas as pl
from jax.experimental.pallas import tpu as pltpu
from jax.sharding import PartitionSpec as P


BF = jnp.bfloat16
F32 = jnp.float32
HI = lax.Precision.HIGHEST

TOK = 128
EXPERTS = 64
CAP = 8
SLOTS = EXPERTS * CAP
WIDTH = 2048
QUART = 512
FF = 256
DK = 128
DV = 256
LANES = 128
HALF = 64


def dot(a, b, ca, cb, precision=None):
    return lax.dot_general(
        a, b, (((ca,), (cb,)), ((), ())), preferred_element_type=F32, precision=precision
    )


def iota(shape, dim):
    return lax.broadcasted_iota(jnp.int32, shape, dim)


def rounded(x):
    return x.astype(BF).astype(F32)


def lower_lanes(shape):
    return iota(shape, len(shape) - 1) < HALF


def call(kernel, out_shape, args, *, index, in_specs=None, flops=0, vmem=24, scratch=()):
    nbytes = sum(a.size * a.dtype.itemsize for a in args)
    nbytes += sum(o.size * o.dtype.itemsize for o in jax.tree.leaves(out_shape))

    def whole(a):
        rank = len(a.shape)
        return pl.BlockSpec(a.shape, lambda i, q: (0,) * rank)

    specs = [whole(a) if s is None else s for a, s in zip(args, in_specs or [None] * len(args))]
    return pl.pallas_call(
        kernel,
        out_shape=out_shape,
        grid_spec=pltpu.PrefetchScalarGridSpec(
            num_scalar_prefetch=1,
            grid=(1,),
            in_specs=specs,
            out_specs=jax.tree.map(whole, out_shape),
            scratch_shapes=scratch,
        ),
        compiler_params=pltpu.CompilerParams(vmem_limit_bytes=vmem * 2**20),
        cost_estimate=pl.CostEstimate(
            flops=int(flops), bytes_accessed=int(nbytes), transcendentals=0
        ),
    )(index, *args)


def in_hbm(a):
    return pltpu.with_memory_space_constraint(a, pltpu.HBM)


def sds(shape, dtype):
    return jax.ShapeDtypeStruct(shape, dtype)


def quarter_rows(q):
    return pl.ds(pl.multiple_of(q * QUART, QUART), QUART)


def cumulative_sum(g):
    lower = (iota((TOK, TOK), 0) >= iota((TOK, TOK), 1)).astype(F32)
    return dot(lower, g, 1, 0, HI)


def tiles_of(state, fill=None):
    out = []
    for b in range(4):
        t = state[:, LANES * (b // 2) : LANES * (b // 2 + 1)]
        r = pltpu.roll(t, HALF, 1)
        low, up = (t, r) if b % 2 == 0 else (r, t)
        upper = fill if fill is not None else up - rounded(up)
        tile = jnp.where(lower_lanes(t.shape), rounded(low), upper)
        out.append(tile.reshape(16, 8, LANES))
    return jnp.concatenate(out, axis=1).reshape(SLOTS, LANES)


def state_of(tiles, upper):
    other = pltpu.roll(tiles, HALF, 1)
    even, odd = (other, tiles) if upper else (tiles, other)
    even, odd = even.reshape(16, 32, LANES), odd.reshape(16, 32, LANES)
    low = lower_lanes((DK, LANES))
    halves = []
    for b in (0, 2):
        first = even[:, 8 * b : 8 * b + 8, :].reshape(DK, LANES)
        second = odd[:, 8 * b + 8 : 8 * b + 16, :].reshape(DK, LANES)
        halves.append(jnp.where(low, first, second))
    return jnp.concatenate(halves, axis=1)


def pick_kernel(q_ref, ids_ref, x_ref, rows_ref, pick_ref, slot_ref):
    expert = iota((EXPERTS, TOK), 0)
    id0, id1 = ids_ref[0:1, :], ids_ref[1:2, :]
    hit0, hit1 = expert == id0, expert == id1
    named = (hit0.astype(F32) + hit1.astype(F32)).astype(BF)
    before = (iota((TOK, TOK), 0) < iota((TOK, TOK), 1)).astype(F32).astype(BF)
    count = dot(named, before, 1, 0)
    rank0 = jnp.sum(jnp.where(hit0, count, 0.0), axis=0, keepdims=True)
    rank1 = jnp.sum(jnp.where(hit1, count, 0.0), axis=0, keepdims=True)
    slot0 = id0 * CAP + rank0.astype(jnp.int32)
    slot1 = id1 * CAP + rank1.astype(jnp.int32)
    slot_ref[0:1, :] = slot0
    slot_ref[1:2, :] = slot1
    slot = iota((SLOTS, TOK), 0)
    pick = ((slot == slot0).astype(F32) + (slot == slot1).astype(F32)).astype(BF)
    pick_ref[...] = pick
    rows_ref[...] = dot(pick, x_ref[...], 1, 0).astype(BF)


def local_kernel(
    q_ref, slot_ref, w_ref, pick_ref, oc_ref, qry_ref, k_ref, v_ref, g_ref,
    rows_ref, tile_ref, cum_ref, dec_ref,
):
    slot = iota((SLOTS, TOK), 0)
    at0, at1 = slot == slot_ref[0:1, :], slot == slot_ref[1:2, :]
    weight = jnp.sum(
        jnp.where(at0, w_ref[0:1, :], 0.0) + jnp.where(at1, w_ref[1:2, :], 0.0),
        axis=1,
        keepdims=True,
    )
    rows_ref[...] = (dot(pick_ref[...], oc_ref[...], 1, 0) * weight).astype(BF)
    g = g_ref[...]
    cum = cumulative_sum(g)
    cum_ref[...] = cum
    dec_ref[...] = qry_ref[...].astype(F32) * jnp.exp(cum)
    to_end = k_ref[...].astype(F32) * jnp.exp(cum[TOK - 1 : TOK, :] - cum)
    state = dot(to_end.T, v_ref[...].astype(F32), 1, 0, HI)
    factor = jnp.exp(jnp.sum(g.T, axis=1, keepdims=True))
    high = rounded(factor)
    fill = jnp.where(iota((DK, LANES), 1) < 96, high, factor - high)
    tile_ref[...] = tiles_of(state, fill).astype(BF)


def gate_kernel(q_ref, x0_ref, x1_ref, x2_ref, x3_ref, wg_ref, wu_ref, g_ref, u_ref):
    g = u = None
    for n, ref in enumerate((x0_ref, x1_ref, x2_ref, x3_ref)):
        rows = quarter_rows(q_ref[n])
        x = ref[...]
        g1, u1 = dot(x, wg_ref[rows, :], 1, 0), dot(x, wu_ref[rows, :], 1, 0)
        g, u = (g1, u1) if g is None else (g + g1, u + u1)
    g_ref[...] = g
    u_ref[...] = u


def near_kernel(q_ref, y0_ref, y1_ref, y2_ref, wd_ref, h_ref):
    h = None
    for n, ref in enumerate((y0_ref, y1_ref, y2_ref)):
        h1 = dot(ref[...], wd_ref[:, quarter_rows(q_ref[n])], 1, 1)
        h = h1 if h is None else h + h1
    h_ref[...] = h


def far_kernel(
    q_ref, g_ref, u_ref, h_ref, top_ref, bot_ref, wg_ref, wu_ref, wd_ref,
    far_ref, right_ref, left_ref, own_ref, hid_ref, gu_ref,
):
    dy = jnp.concatenate([top_ref[...], bot_ref[...]], axis=0)
    g, u = g_ref[...], u_ref[...]
    h = h_ref[...] + dot(dy, wd_ref[:, quarter_rows(q_ref[3])], 1, 1)
    sig = jax.nn.sigmoid(g)
    hid_ref[...] = (g * sig * u).astype(BF)
    gate_cot = (h * u * sig * (1.0 + g * (1.0 - sig))).astype(BF)
    up_cot = (h * g * sig).astype(BF)
    gu_ref[:, :FF] = gate_cot
    gu_ref[:, FF:] = up_cot
    for n, ref in ((3, far_ref), (2, right_ref), (1, left_ref), (0, own_ref)):
        rows = quarter_rows(q_ref[n])
        part = dot(gate_cot, wg_ref[rows, :], 1, 1) + dot(up_cot, wu_ref[rows, :], 1, 1)
        ref[...] = part.astype(BF)


def weight_kernel(
    q_ref, x0_ref, x1_ref, x2_ref, x3_ref, y0_ref, y1_ref, y2_ref, top_ref, bot_ref,
    hid_ref, gu_ref, gg_ref, gup_ref, gd_ref,
):
    hid_t = hid_ref[...].T
    gu = gu_ref[...]
    far = jnp.concatenate([top_ref[...], bot_ref[...]], axis=0)
    cots = (y0_ref[...], y1_ref[...], y2_ref[...], far)
    for n, ref in enumerate((x0_ref, x1_ref, x2_ref, x3_ref)):
        rows = quarter_rows(q_ref[n])
        both = dot(ref[...].T, gu, 1, 0)
        gg_ref[rows, :] = both[:, :FF]
        gup_ref[rows, :] = both[:, FF:]
        gd_ref[:, rows] = dot(hid_t, cots[n], 1, 0)


def sum_kernel(q_ref, p0_ref, p1_ref, p2_ref, p3_ref, out_ref):
    total = p0_ref[...].astype(F32) + p1_ref[...].astype(F32)
    out_ref[...] = (total + p2_ref[...].astype(F32) + p3_ref[...].astype(F32)).astype(BF)


def combine_kernel(q_ref, rows_ref, pick_ref, oc_ref, out_ref):
    routed = dot(pick_ref[...].T, rows_ref[...], 1, 0)
    out_ref[...] = (oc_ref[...].astype(F32) + routed).astype(BF)


def head_kernel(
    q_ref, m0_ref, m1_ref, m2_ref, m3_ref, w_ref, dec_ref, tile_ref, h_ref, pay_ref
):
    head = None
    for n, ref in enumerate((m0_ref, m1_ref, m2_ref, m3_ref)):
        part = dot(ref[...], w_ref[quarter_rows(q_ref[n]), :], 1, 0)
        head = part if head is None else head + part
    h_ref[...] = head
    pay_ref[:, :LANES] = tiles_of(dot(dec_ref[...].T, head, 1, 0, HI)).astype(BF)
    pay_ref[:, LANES:] = tile_ref[...]


def out_proj_kernel(q_ref, m0_ref, m1_ref, m2_ref, m3_ref, mixed_ref, keep_ref, give_ref):
    mixed = mixed_ref[...]
    first = q_ref[4] == 0
    for n, ref in enumerate((m0_ref, m1_ref, m2_ref, m3_ref)):
        part = dot(ref[...].T, mixed, 1, 0).reshape(16, 32, DV)
        low = part[:, :16, :].reshape(256, DV)
        high = part[:, 16:, :].reshape(256, DV)
        rows = pl.ds(pl.multiple_of(q_ref[n] * 256, 256), 256)
        keep_ref[rows, :] = jnp.where(first, low, high).astype(BF)
        give_ref[rows, :] = jnp.where(first, high, low).astype(BF)


def split_kernel(q_ref, keep_ref, got_ref, o0_ref, o1_ref, o2_ref, o3_ref):
    total = (keep_ref[...].astype(F32) + got_ref[...].astype(F32)).reshape(64, 16, DV)
    tile = [
        total[:, 8 * (n // 2) : 8 * (n // 2) + 8, LANES * (n % 2) : LANES * (n % 2) + LANES]
        for n in range(4)
    ]
    tile = [t.reshape(SLOTS, LANES) for t in tile]
    y = q_ref[5]
    for k, ref in enumerate((o0_ref, o1_ref, o2_ref, o3_ref)):
        out = tile[k]
        for n in range(1, 4):
            out = jnp.where(y == n, tile[(n + k) % 4], out)
        ref[...] = out.astype(BF)


def scan_kernel(
    q_ref, in_ref, o_ref, r1_ref, r2_ref, r3_ref, out_ref, factor_ref, pre_ref, suf_ref
):
    pull = in_ref[:, :LANES].astype(F32)
    suf_ref[...] = pull + pltpu.roll(pull, HALF, 1)
    tile = in_ref[:, LANES:].astype(F32)
    pre_ref[...] = pltpu.roll(tile, HALF, 1)
    factor_ref[...] = jnp.broadcast_to(tile[:, 64:65] + tile[:, 96:97], tile.shape)
    before = after = jnp.zeros((8, LANES), F32)
    for s in range(EXPERTS):
        rows = slice(8 * s, 8 * s + 8)
        now = pre_ref[rows, :]
        pre_ref[rows, :] = before
        before = before * factor_ref[rows, :] + now
        e = EXPERTS - 1 - s
        rows = slice(8 * e, 8 * e + 8)
        now = suf_ref[rows, :]
        suf_ref[rows, :] = after
        after = after * factor_ref[rows, :] + now
    suf = suf_ref[...]
    out_ref[:, :LANES] = jnp.where(lower_lanes(suf.shape), suf, pre_ref[...]).astype(BF)
    total = o_ref[...].astype(F32) + r1_ref[...].astype(F32)
    out_ref[:, LANES:] = (total + r2_ref[...].astype(F32) + r3_ref[...].astype(F32)).astype(BF)


def inside_kernel(
    q_ref, k_ref, v_ref, cum_ref, dec_ref, h_ref, dq_ref, dk_ref, dv_ref
):
    k, v, q_dec, head = k_ref[...].astype(F32), v_ref[...].astype(F32), dec_ref[...], h_ref[...]
    k_grown = k * jnp.exp(-cum_ref[...])
    causal = iota((TOK, TOK), 0) >= iota((TOK, TOK), 1)
    score = jnp.where(causal, dot(q_dec, k_grown, 1, 1, HI), 0.0)
    d_score = jnp.where(causal, dot(head, v, 1, 1, HI), 0.0)
    dq_ref[...] = dot(d_score, k_grown, 1, 0, HI)
    dk_ref[...] = dot(d_score.T, q_dec, 1, 0, HI)
    dv_ref[...] = dot(score.T, head, 1, 0, HI)


def last_kernel(
    q_ref, k_ref, v_ref, cum_ref, dec_ref, h_ref, dq_ref, dk_ref, dv_ref, in_ref,
    gq_ref, gk_ref, gv_ref, gg_ref, go_ref,
):
    tiles = in_ref[:, :LANES].astype(F32)
    cot, state = state_of(tiles, False), state_of(tiles, True)
    k, v, head, cum = k_ref[...].astype(F32), v_ref[...].astype(F32), h_ref[...], cum_ref[...]
    last = cum[TOK - 1 : TOK, :]
    shrink, to_end = jnp.exp(-cum), jnp.exp(last - cum)
    k_end = k * to_end
    d_q = dq_ref[...] + dot(head, state, 1, 1, HI)
    d_kg = dk_ref[...]
    d_ke = dot(v, cot, 1, 1, HI)
    gq_ref[...] = (d_q * jnp.exp(cum)).astype(BF)
    gk_ref[...] = (d_kg * shrink + d_ke * to_end).astype(BF)
    gv_ref[...] = (dv_ref[...] + dot(k_end, cot, 1, 0, HI)).astype(BF)
    end = d_ke * k_end
    d_cum = d_q * dec_ref[...] - d_kg * (k * shrink) - end
    carried = jnp.sum((state * cot).T, axis=0, keepdims=True)
    d_last = jnp.sum(end, axis=0, keepdims=True) + jnp.exp(last) * carried
    upper = (iota((TOK, TOK), 0) <= iota((TOK, TOK), 1)).astype(F32)
    gg_ref[...] = dot(upper, d_cum, 1, 0, HI) + d_last
    parts = jnp.sum(in_ref[:, LANES:].astype(F32).reshape(8, EXPERTS, LANES), axis=0)
    for y in range(4):
        for core in range(2):
            n = 8 * (2 * y + core)
            rows = 16 * core + 8 * (y // 2)
            lanes = LANES * (y % 2)
            go_ref[rows : rows + 8, lanes : lanes + LANES] = parts[n : n + 8, :]


def per_device(
    expert_in, out_cot, route_ids, route_weights, w_gate, w_up, w_down, w_out,
    mixed_heads, queries, keys, values, log_decay,
):
    me, sp = lax.axis_index("tp"), lax.axis_index("sp")
    table = [
        [i, (i + 3) % 4, (i + 1) % 4, (i + 2) % 4, s % 2, s // 2] for s in range(8) for i in range(4)
    ]
    place = lax.rem(sp, 8) * 4 + me
    order = lax.dynamic_slice(jnp.array(table, jnp.int32).reshape(-1), (place * 6,), (6,))
    to_right = [(i, (i + 1) % 4) for i in range(4)]
    to_left = [(i, (i + 3) % 4) for i in range(4)]
    across = [(i, (i + 2) % 4) for i in range(4)]
    other_core = [(i, i ^ 1) for i in range(64)]

    def along_y(k):
        return [(i, i // 8 * 8 + (i + 2 * k) % 8) for i in range(64)]

    wg, wu, wd = w_gate[0], w_up[0], w_down[0]
    run = functools.partial(call, index=order)

    def exchange(rows):
        width = rows.shape[1]
        got = lax.all_to_all(rows.reshape(EXPERTS, CAP, width), "sp", 0, 0, tiled=True)
        return got.reshape(SLOTS, width)

    def quarter_block():
        return pl.BlockSpec((TOK, QUART), lambda i, q: (0, q[0]))

    rows_type = sds((SLOTS, QUART), BF)
    tile_type = sds((SLOTS, LANES), BF)
    x_rows, pick, slots = run(
        pick_kernel,
        (rows_type, sds((SLOTS, TOK), BF), sds((2, TOK), jnp.int32)),
        (route_ids.T, in_hbm(expert_in)),
        in_specs=[None, quarter_block()],
        flops=1e8,
    )
    y_rows, state_tile, cum, q_dec = run(
        local_kernel,
        (rows_type, tile_type, sds((TOK, DK), F32), sds((TOK, DK), F32)),
        (
            slots, route_weights.T, pick, in_hbm(out_cot), in_hbm(queries), in_hbm(keys),
            in_hbm(values), in_hbm(log_decay),
        ),
        in_specs=[None, None, None, quarter_block(), None, None, None, None],
        flops=3e8,
    )
    x0 = exchange(x_rows)
    x0, y_rows = lax.optimization_barrier((x0, y_rows))
    x3 = lax.ppermute(x0, "tp", across)
    x1 = lax.ppermute(x0, "tp", to_right)
    x2 = lax.ppermute(x0, "tp", to_left)
    y0 = exchange(y_rows)
    y1 = lax.ppermute(y0, "tp", to_right)
    y2 = lax.ppermute(y0, "tp", to_left)
    far_top = lax.ppermute(y1[: SLOTS // 2], "tp", to_right)
    far_bottom = lax.ppermute(y2[SLOTS // 2 :], "tp", to_left)
    g, u = run(
        gate_kernel, (sds((SLOTS, FF), F32),) * 2, (x0, x1, x2, x3, wg, wu), flops=1.1e9
    )
    h = run(near_kernel, sds((SLOTS, FF), F32), (y0, y1, y2, wd), flops=4e8)
    p_far, p_right, p_left, p_own, hidden, gate_up = run(
        far_kernel,
        (rows_type,) * 4 + (sds((SLOTS, FF), BF), sds((SLOTS, 2 * FF), BF)),
        (g, u, h, far_top, far_bottom, wg, wu, wd),
        flops=1.3e9,
    )
    r_far = lax.ppermute(p_far, "tp", across)
    r_left = lax.ppermute(p_right, "tp", to_right)
    r_right = lax.ppermute(p_left, "tp", to_left)
    grads = run(
        weight_kernel,
        (sds((WIDTH, FF), F32), sds((WIDTH, FF), F32), sds((FF, WIDTH), F32)),
        (x0, x1, x2, x3, y0, y1, y2, far_top, far_bottom, hidden, gate_up),
        flops=1.6e9,
    )
    p_own, grads = lax.optimization_barrier((p_own, grads))
    grad_gate, grad_up, grad_down = grads
    total = run(sum_kernel, rows_type, (p_own, r_far, r_left, r_right), flops=1e6)
    back = exchange(total)
    mid = run(
        combine_kernel,
        sds((TOK, QUART), BF),
        (back, pick, out_cot),
        in_specs=[None, None, quarter_block()],
        flops=7e7,
    )
    m_far = lax.ppermute(mid, "tp", across)
    m_left = lax.ppermute(mid, "tp", to_right)
    m_right = lax.ppermute(mid, "tp", to_left)
    mids = (mid, m_left, m_right, m_far)
    head, pay = run(
        head_kernel,
        (sds((TOK, DV), F32), sds((SLOTS, 2 * LANES), BF)),
        (*mids, w_out, q_dec, state_tile),
        flops=2e8,
    )
    pulled = exchange(pay)
    keep, give = run(out_proj_kernel, (sds((1024, DV), BF),) * 2, (*mids, mixed_heads), flops=1.4e8)
    got = lax.ppermute(give, "sp", other_core)
    tiles = run(split_kernel, (tile_type,) * 4, (keep, got), flops=1e6)
    adds = [lax.ppermute(tiles[k], "sp", along_y(k)) for k in (2, 1, 3)]
    pay = run(
        scan_kernel,
        sds((SLOTS, 2 * LANES), BF),
        (pulled, tiles[0], *adds),
        flops=1e8,
        scratch=[pltpu.VMEM((SLOTS, LANES), F32)] * 3,
    )
    back_states = exchange(pay)
    d_in = run(
        inside_kernel,
        (sds((TOK, DK), F32), sds((TOK, DK), F32), sds((TOK, DV), F32)),
        (keys, values, cum, q_dec, head),
        flops=3e8,
    )
    grad_queries, grad_keys, grad_values, grad_decay, grad_out_proj = run(
        last_kernel,
        (
            sds((TOK, DK), BF),
            sds((TOK, DK), BF),
            sds((TOK, DV), BF),
            sds((TOK, DK), F32),
            sds((32, DV), F32),
        ),
        (keys, values, cum, q_dec, head, *d_in, back_states),
        flops=3e8,
    )
    return (
        grad_gate[None],
        grad_up[None],
        grad_down[None],
        grad_out_proj,
        grad_queries,
        grad_keys,
        grad_values,
        grad_decay,
    )


def solution(mesh):
    return jax.shard_map(
        per_device,
        mesh=mesh,
        in_specs=(
            P("sp", None),
            P("sp", None),
            P("sp", None),
            P("sp", None),
            P("sp", None, "tp"),
            P("sp", None, "tp"),
            P("sp", "tp", None),
            P(None, "tp"),
            P("sp", "tp"),
            P("sp", "tp"),
            P("sp", "tp"),
            P("sp", "tp"),
            P("sp", "tp"),
        ),
        out_specs=(
            P("sp", None, "tp"),
            P("sp", None, "tp"),
            P("sp", "tp", None),
            P("sp", "tp"),
            P("sp", "tp"),
            P("sp", "tp"),
            P("sp", "tp"),
            P("sp", "tp"),
        ),
        check_vma=False,
    )
```

```python
import functools

import jax
import jax.numpy as jnp
from jax import lax
from jax.experimental import pallas as pl
from jax.experimental.pallas import tpu as pltpu
from jax.sharding import PartitionSpec as P


BF = jnp.bfloat16
F32 = jnp.float32
HI = lax.Precision.HIGHEST

TOK = 128
EXPERTS = 64
CAP = 8
SLOTS = EXPERTS * CAP
WIDTH = 2048
QUART = 512
FF = 256
DK = 128
DV = 256
LANES = 128
HALF = 64


def dot(a, b, ca, cb, precision=None):
    return lax.dot_general(
        a, b, (((ca,), (cb,)), ((), ())), preferred_element_type=F32, precision=precision
    )


def iota(shape, dim):
    return lax.broadcasted_iota(jnp.int32, shape, dim)


def rounded(x):
    return x.astype(BF).astype(F32)


def lower_lanes(shape):
    return iota(shape, len(shape) - 1) < HALF


def call(kernel, out_shape, args, *, index, in_specs=None, flops=0, vmem=24, scratch=()):
    nbytes = sum(a.size * a.dtype.itemsize for a in args)
    nbytes += sum(o.size * o.dtype.itemsize for o in jax.tree.leaves(out_shape))

    def whole(a):
        rank = len(a.shape)
        return pl.BlockSpec(a.shape, lambda i, q: (0,) * rank)

    specs = [whole(a) if s is None else s for a, s in zip(args, in_specs or [None] * len(args))]
    return pl.pallas_call(
        kernel,
        out_shape=out_shape,
        grid_spec=pltpu.PrefetchScalarGridSpec(
            num_scalar_prefetch=1,
            grid=(1,),
            in_specs=specs,
            out_specs=jax.tree.map(whole, out_shape),
            scratch_shapes=scratch,
        ),
        compiler_params=pltpu.CompilerParams(vmem_limit_bytes=vmem * 2**20),
        cost_estimate=pl.CostEstimate(
            flops=int(flops), bytes_accessed=int(nbytes), transcendentals=0
        ),
    )(index, *args)


def in_hbm(a):
    return pltpu.with_memory_space_constraint(a, pltpu.HBM)


def sds(shape, dtype):
    return jax.ShapeDtypeStruct(shape, dtype)


def quarter_rows(q):
    return pl.ds(pl.multiple_of(q * QUART, QUART), QUART)


def cumulative_sum(g):
    lower = (iota((TOK, TOK), 0) >= iota((TOK, TOK), 1)).astype(F32)
    return dot(lower, g, 1, 0, HI)


def tiles_of(state, fill=None):
    out = []
    for b in range(4):
        t = state[:, LANES * (b // 2) : LANES * (b // 2 + 1)]
        r = pltpu.roll(t, HALF, 1)
        low, up = (t, r) if b % 2 == 0 else (r, t)
        upper = fill if fill is not None else up - rounded(up)
        tile = jnp.where(lower_lanes(t.shape), rounded(low), upper)
        out.append(tile.reshape(16, 8, LANES))
    return jnp.concatenate(out, axis=1).reshape(SLOTS, LANES)


def state_of(tiles, upper):
    other = pltpu.roll(tiles, HALF, 1)
    even, odd = (other, tiles) if upper else (tiles, other)
    even, odd = even.reshape(16, 32, LANES), odd.reshape(16, 32, LANES)
    low = lower_lanes((DK, LANES))
    halves = []
    for b in (0, 2):
        first = even[:, 8 * b : 8 * b + 8, :].reshape(DK, LANES)
        second = odd[:, 8 * b + 8 : 8 * b + 16, :].reshape(DK, LANES)
        halves.append(jnp.where(low, first, second))
    return jnp.concatenate(halves, axis=1)


def pick_kernel(q_ref, ids_ref, x_ref, rows_ref, pick_ref, slot_ref):
    expert = iota((EXPERTS, TOK), 0)
    id0, id1 = ids_ref[0:1, :], ids_ref[1:2, :]
    hit0, hit1 = expert == id0, expert == id1
    named = (hit0.astype(F32) + hit1.astype(F32)).astype(BF)
    before = (iota((TOK, TOK), 0) < iota((TOK, TOK), 1)).astype(F32).astype(BF)
    count = dot(named, before, 1, 0)
    rank0 = jnp.sum(jnp.where(hit0, count, 0.0), axis=0, keepdims=True)
    rank1 = jnp.sum(jnp.where(hit1, count, 0.0), axis=0, keepdims=True)
    slot0 = id0 * CAP + rank0.astype(jnp.int32)
    slot1 = id1 * CAP + rank1.astype(jnp.int32)
    slot_ref[0:1, :] = slot0
    slot_ref[1:2, :] = slot1
    slot = iota((SLOTS, TOK), 0)
    pick = ((slot == slot0).astype(F32) + (slot == slot1).astype(F32)).astype(BF)
    pick_ref[...] = pick
    rows_ref[...] = dot(pick, x_ref[...], 1, 0).astype(BF)


def local_kernel(
    q_ref, slot_ref, w_ref, pick_ref, oc_ref, qry_ref, k_ref, v_ref, g_ref,
    rows_ref, tile_ref, cum_ref, dec_ref,
):
    slot = iota((SLOTS, TOK), 0)
    at0, at1 = slot == slot_ref[0:1, :], slot == slot_ref[1:2, :]
    weight = jnp.sum(
        jnp.where(at0, w_ref[0:1, :], 0.0) + jnp.where(at1, w_ref[1:2, :], 0.0),
        axis=1,
        keepdims=True,
    )
    rows_ref[...] = (dot(pick_ref[...], oc_ref[...], 1, 0) * weight).astype(BF)
    g = g_ref[...]
    cum = cumulative_sum(g)
    cum_ref[...] = cum
    dec_ref[...] = qry_ref[...].astype(F32) * jnp.exp(cum)
    to_end = k_ref[...].astype(F32) * jnp.exp(cum[TOK - 1 : TOK, :] - cum)
    state = dot(to_end.T, v_ref[...].astype(F32), 1, 0, HI)
    factor = jnp.exp(jnp.sum(g.T, axis=1, keepdims=True))
    high = rounded(factor)
    fill = jnp.where(iota((DK, LANES), 1) < 96, high, factor - high)
    tile_ref[...] = tiles_of(state, fill).astype(BF)


def gate_near_kernel(q_ref, x0_ref, x1_ref, x2_ref, wg_ref, wu_ref, g_ref, u_ref):
    g = u = None
    for n, ref in enumerate((x0_ref, x1_ref, x2_ref)):
        rows = quarter_rows(q_ref[n])
        x = ref[...]
        g1, u1 = dot(x, wg_ref[rows, :], 1, 0), dot(x, wu_ref[rows, :], 1, 0)
        g, u = (g1, u1) if g is None else (g + g1, u + u1)
    g_ref[...] = g
    u_ref[...] = u


def gate_far_kernel(
    q_ref, g_ref, u_ref, t3_ref, b3_ref, wg_ref, wu_ref, hid_ref, to_gate_ref, to_up_ref
):
    rows = quarter_rows(q_ref[3])
    x = jnp.concatenate([t3_ref[...], b3_ref[...]], axis=0)
    g = g_ref[...] + dot(x, wg_ref[rows, :], 1, 0)
    u = u_ref[...] + dot(x, wu_ref[rows, :], 1, 0)
    sig = jax.nn.sigmoid(g)
    silu = g * sig
    hid_ref[...] = (silu * u).astype(BF)
    to_gate_ref[...] = u * sig * (1.0 + g * (1.0 - sig))
    to_up_ref[...] = silu


TOP, BOTTOM = slice(0, SLOTS // 2), slice(SLOTS // 2, SLOTS)


def near_kernel(q_ref, y0_ref, t1_ref, b1_ref, t2_ref, b2_ref, wd_ref, h_ref):
    w0, w1, w2 = (wd_ref[:, quarter_rows(q_ref[n])] for n in range(3))
    h = dot(y0_ref[...], w0, 1, 1)
    h_ref[TOP, :] = h[TOP] + dot(t1_ref[...], w1, 1, 1) + dot(t2_ref[...], w2, 1, 1)
    h_ref[BOTTOM, :] = h[BOTTOM] + dot(b1_ref[...], w1, 1, 1) + dot(b2_ref[...], w2, 1, 1)


def back_rows(gu_ref, wg_ref, wu_ref, rows):
    part = dot(gu_ref[:, :FF], wg_ref[rows, :], 1, 1) + dot(gu_ref[:, FF:], wu_ref[rows, :], 1, 1)
    return part.astype(BF)


def far_kernel(
    q_ref, h_ref, t3_ref, b3_ref, to_gate_ref, to_up_ref, wg_ref, wu_ref, wd_ref,
    gu_ref, top_ref, bottom_ref,
):
    w3 = wd_ref[:, quarter_rows(q_ref[3])]
    for rows, ref in ((TOP, t3_ref), (BOTTOM, b3_ref)):
        h = h_ref[rows, :] + dot(ref[...], w3, 1, 1)
        gu_ref[rows, :FF] = (h * to_gate_ref[rows, :]).astype(BF)
        gu_ref[rows, FF:] = (h * to_up_ref[rows, :]).astype(BF)
    far = back_rows(gu_ref, wg_ref, wu_ref, quarter_rows(q_ref[3]))
    top_ref[...] = far[TOP]
    bottom_ref[...] = far[BOTTOM]


def sides_kernel(q_ref, gu_ref, wg_ref, wu_ref, rt_ref, rb_ref, lt_ref, lb_ref):
    for n, top_ref, bottom_ref in ((2, rt_ref, rb_ref), (1, lt_ref, lb_ref)):
        part = back_rows(gu_ref, wg_ref, wu_ref, quarter_rows(q_ref[n]))
        top_ref[...] = part[TOP]
        bottom_ref[...] = part[BOTTOM]


def merge_kernel(q_ref, rt_ref, lb_ref, from_left_ref, from_right_ref, t_ref, b_ref):
    t_ref[...] = (rt_ref[...].astype(F32) + from_left_ref[...].astype(F32)).astype(BF)
    b_ref[...] = (lb_ref[...].astype(F32) + from_right_ref[...].astype(F32)).astype(BF)


def weight_kernel(
    q_ref, x0_ref, x1_ref, x2_ref, xt_ref, xb_ref,
    y0_ref, t1_ref, b1_ref, t2_ref, b2_ref, t3_ref, b3_ref,
    hid_ref, gu_ref, wg_ref, wu_ref, gg_ref, gup_ref, gd_ref, own_ref,
):
    own_ref[...] = back_rows(gu_ref, wg_ref, wu_ref, quarter_rows(q_ref[0]))
    hid_t = hid_ref[...].T
    gu = gu_ref[...]
    pairs = ((t1_ref, b1_ref), (t2_ref, b2_ref), (t3_ref, b3_ref))
    cots = [y0_ref[...]] + [jnp.concatenate([t[...], b[...]], axis=0) for t, b in pairs]
    far = jnp.concatenate([xt_ref[...], xb_ref[...]], axis=0)
    for n, x in enumerate((x0_ref[...], x1_ref[...], x2_ref[...], far)):
        rows = quarter_rows(q_ref[n])
        both = dot(x.T, gu, 1, 0)
        gg_ref[rows, :] = both[:, :FF]
        gup_ref[rows, :] = both[:, FF:]
        gd_ref[:, rows] = dot(hid_t, cots[n], 1, 0)


def sum_kernel(q_ref, own_ref, tl_ref, tr_ref, bl_ref, br_ref, out_ref):
    for rows, a_ref, b_ref in ((TOP, tl_ref, tr_ref), (BOTTOM, bl_ref, br_ref)):
        got = a_ref[...].astype(F32) + b_ref[...].astype(F32)
        out_ref[rows, :] = (own_ref[rows, :].astype(F32) + got).astype(BF)


def combine_kernel(q_ref, rows_ref, pick_ref, oc_ref, out_ref):
    routed = dot(pick_ref[...].T, rows_ref[...], 1, 0)
    out_ref[...] = (oc_ref[...].astype(F32) + routed).astype(BF)


def head_kernel(
    q_ref, m0_ref, m1_ref, m2_ref, m3_ref, w_ref, dec_ref, tile_ref, h_ref, pay_ref
):
    head = None
    for n, ref in enumerate((m0_ref, m1_ref, m2_ref, m3_ref)):
        part = dot(ref[...], w_ref[quarter_rows(q_ref[n]), :], 1, 0)
        head = part if head is None else head + part
    h_ref[...] = head
    pay_ref[:, :LANES] = tiles_of(dot(dec_ref[...].T, head, 1, 0, HI)).astype(BF)
    pay_ref[:, LANES:] = tile_ref[...]


def out_proj_kernel(q_ref, m0_ref, m1_ref, m2_ref, m3_ref, mixed_ref, keep_ref, give_ref):
    mixed = mixed_ref[...]
    first = q_ref[4] == 0
    for n, ref in enumerate((m0_ref, m1_ref, m2_ref, m3_ref)):
        part = dot(ref[...].T, mixed, 1, 0).reshape(16, 32, DV)
        low = part[:, :16, :].reshape(256, DV)
        high = part[:, 16:, :].reshape(256, DV)
        rows = pl.ds(pl.multiple_of(q_ref[n] * 256, 256), 256)
        keep_ref[rows, :] = jnp.where(first, low, high).astype(BF)
        give_ref[rows, :] = jnp.where(first, high, low).astype(BF)


def split_kernel(q_ref, keep_ref, got_ref, o0_ref, o1_ref, o2_ref, o3_ref):
    total = (keep_ref[...].astype(F32) + got_ref[...].astype(F32)).reshape(64, 16, DV)
    tile = [
        total[:, 8 * (n // 2) : 8 * (n // 2) + 8, LANES * (n % 2) : LANES * (n % 2) + LANES]
        for n in range(4)
    ]
    tile = [t.reshape(SLOTS, LANES) for t in tile]
    y = q_ref[5]
    for k, ref in enumerate((o0_ref, o1_ref, o2_ref, o3_ref)):
        out = tile[k]
        for n in range(1, 4):
            out = jnp.where(y == n, tile[(n + k) % 4], out)
        ref[...] = out.astype(BF)


def scan_kernel(
    q_ref, in_ref, o_ref, r1_ref, r2_ref, r3_ref, out_ref, factor_ref, pre_ref, suf_ref
):
    pull = in_ref[:, :LANES].astype(F32)
    suf_ref[...] = pull + pltpu.roll(pull, HALF, 1)
    tile = in_ref[:, LANES:].astype(F32)
    pre_ref[...] = pltpu.roll(tile, HALF, 1)
    factor_ref[...] = jnp.broadcast_to(tile[:, 64:65] + tile[:, 96:97], tile.shape)
    before = after = jnp.zeros((8, LANES), F32)
    for s in range(EXPERTS):
        rows = slice(8 * s, 8 * s + 8)
        now = pre_ref[rows, :]
        pre_ref[rows, :] = before
        before = before * factor_ref[rows, :] + now
        e = EXPERTS - 1 - s
        rows = slice(8 * e, 8 * e + 8)
        now = suf_ref[rows, :]
        suf_ref[rows, :] = after
        after = after * factor_ref[rows, :] + now
    suf = suf_ref[...]
    out_ref[:, :LANES] = jnp.where(lower_lanes(suf.shape), suf, pre_ref[...]).astype(BF)
    total = o_ref[...].astype(F32) + r1_ref[...].astype(F32)
    out_ref[:, LANES:] = (total + r2_ref[...].astype(F32) + r3_ref[...].astype(F32)).astype(BF)


def inside_kernel(
    q_ref, k_ref, v_ref, cum_ref, dec_ref, h_ref, dq_ref, dk_ref, dv_ref
):
    k, v, q_dec, head = k_ref[...].astype(F32), v_ref[...].astype(F32), dec_ref[...], h_ref[...]
    k_grown = k * jnp.exp(-cum_ref[...])
    causal = iota((TOK, TOK), 0) >= iota((TOK, TOK), 1)
    score = jnp.where(causal, dot(q_dec, k_grown, 1, 1, HI), 0.0)
    d_score = jnp.where(causal, dot(head, v, 1, 1, HI), 0.0)
    dq_ref[...] = dot(d_score, k_grown, 1, 0, HI)
    dk_ref[...] = dot(d_score.T, q_dec, 1, 0, HI)
    dv_ref[...] = dot(score.T, head, 1, 0, HI)


def last_kernel(
    q_ref, k_ref, v_ref, cum_ref, dec_ref, h_ref, dq_ref, dk_ref, dv_ref, in_ref,
    gq_ref, gk_ref, gv_ref, gg_ref, go_ref,
):
    tiles = in_ref[:, :LANES].astype(F32)
    cot, state = state_of(tiles, False), state_of(tiles, True)
    k, v, head, cum = k_ref[...].astype(F32), v_ref[...].astype(F32), h_ref[...], cum_ref[...]
    last = cum[TOK - 1 : TOK, :]
    shrink, to_end = jnp.exp(-cum), jnp.exp(last - cum)
    k_end = k * to_end
    d_q = dq_ref[...] + dot(head, state, 1, 1, HI)
    d_kg = dk_ref[...]
    d_ke = dot(v, cot, 1, 1, HI)
    gq_ref[...] = (d_q * jnp.exp(cum)).astype(BF)
    gk_ref[...] = (d_kg * shrink + d_ke * to_end).astype(BF)
    gv_ref[...] = (dv_ref[...] + dot(k_end, cot, 1, 0, HI)).astype(BF)
    end = d_ke * k_end
    d_cum = d_q * dec_ref[...] - d_kg * (k * shrink) - end
    carried = jnp.sum((state * cot).T, axis=0, keepdims=True)
    d_last = jnp.sum(end, axis=0, keepdims=True) + jnp.exp(last) * carried
    upper = (iota((TOK, TOK), 0) <= iota((TOK, TOK), 1)).astype(F32)
    gg_ref[...] = dot(upper, d_cum, 1, 0, HI) + d_last
    parts = jnp.sum(in_ref[:, LANES:].astype(F32).reshape(8, EXPERTS, LANES), axis=0)
    for y in range(4):
        for core in range(2):
            n = 8 * (2 * y + core)
            rows = 16 * core + 8 * (y // 2)
            lanes = LANES * (y % 2)
            go_ref[rows : rows + 8, lanes : lanes + LANES] = parts[n : n + 8, :]


def per_device(
    expert_in, out_cot, route_ids, route_weights, w_gate, w_up, w_down, w_out,
    mixed_heads, queries, keys, values, log_decay,
):
    me, sp = lax.axis_index("tp"), lax.axis_index("sp")
    table = [
        [i, (i + 3) % 4, (i + 1) % 4, (i + 2) % 4, s % 2, s // 2] for s in range(8) for i in range(4)
    ]
    place = lax.rem(sp, 8) * 4 + me
    order = lax.dynamic_slice(jnp.array(table, jnp.int32).reshape(-1), (place * 6,), (6,))
    to_right = [(i, (i + 1) % 4) for i in range(4)]
    to_left = [(i, (i + 3) % 4) for i in range(4)]
    across = [(i, (i + 2) % 4) for i in range(4)]
    other_core = [(i, i ^ 1) for i in range(64)]

    def along_y(k):
        return [(i, i // 8 * 8 + (i + 2 * k) % 8) for i in range(64)]

    wg, wu, wd = w_gate[0], w_up[0], w_down[0]
    run = functools.partial(call, index=order)

    def exchange(rows):
        width = rows.shape[1]
        got = lax.all_to_all(rows.reshape(EXPERTS, CAP, width), "sp", 0, 0, tiled=True)
        return got.reshape(SLOTS, width)

    def quarter_block():
        return pl.BlockSpec((TOK, QUART), lambda i, q: (0, q[0]))

    rows_type = sds((SLOTS, QUART), BF)
    tile_type = sds((SLOTS, LANES), BF)
    x_rows, pick, slots = run(
        pick_kernel,
        (rows_type, sds((SLOTS, TOK), BF), sds((2, TOK), jnp.int32)),
        (in_hbm(route_ids.T), in_hbm(expert_in)),
        in_specs=[None, quarter_block()],
        flops=1e8,
    )
    y_rows, state_tile, cum, q_dec = run(
        local_kernel,
        (rows_type, tile_type, sds((TOK, DK), F32), sds((TOK, DK), F32)),
        (
            slots, in_hbm(route_weights.T), pick, in_hbm(out_cot), in_hbm(queries), in_hbm(keys),
            in_hbm(values), in_hbm(log_decay),
        ),
        in_specs=[None, None, None, quarter_block(), None, None, None, None],
        flops=3e8,
    )
    x0 = exchange(x_rows)
    x0, y_rows = lax.optimization_barrier((x0, y_rows))
    x1 = lax.ppermute(x0, "tp", to_right)
    x2 = lax.ppermute(x0, "tp", to_left)
    xt3 = lax.ppermute(x1[TOP], "tp", to_right)
    xb3 = lax.ppermute(x2[BOTTOM], "tp", to_left)
    y0 = exchange(y_rows)
    y_top, y_bottom = y0[TOP], y0[BOTTOM]
    t1 = lax.ppermute(y_top, "tp", to_right)
    b2 = lax.ppermute(y_bottom, "tp", to_left)
    b1 = lax.ppermute(y_bottom, "tp", to_right)
    t2 = lax.ppermute(y_top, "tp", to_left)
    t3 = lax.ppermute(t1, "tp", to_right)
    b3 = lax.ppermute(b2, "tp", to_left)
    half_type = sds((SLOTS, FF), F32)
    part_type = sds((SLOTS // 2, QUART), BF)
    g, u = run(gate_near_kernel, (half_type,) * 2, (x0, x1, x2, wg, wu), flops=8e8)
    hidden, to_gate, to_up = run(
        gate_far_kernel,
        (sds((SLOTS, FF), BF), half_type, half_type),
        (g, u, xt3, xb3, wg, wu),
        flops=3e8,
    )
    h = run(near_kernel, half_type, (y0, t1, b1, t2, b2, wd), flops=4e8)
    gate_up, p_top, p_bottom = run(
        far_kernel,
        (sds((SLOTS, 2 * FF), BF), part_type, part_type),
        (h, t3, b3, to_gate, to_up, wg, wu, wd),
        flops=4e8,
    )
    far_top = lax.ppermute(p_top, "tp", to_right)
    far_bottom = lax.ppermute(p_bottom, "tp", to_left)
    p_rt, p_rb, p_lt, p_lb = run(sides_kernel, (part_type,) * 4, (gate_up, wg, wu), flops=5e8)
    bl = lax.ppermute(p_rb, "tp", to_right)
    tr = lax.ppermute(p_lt, "tp", to_left)
    p_t, p_b = run(merge_kernel, (part_type,) * 2, (p_rt, p_lb, far_top, far_bottom), flops=1e6)
    tl = lax.ppermute(p_t, "tp", to_right)
    br = lax.ppermute(p_b, "tp", to_left)
    *grads, p_own = run(
        weight_kernel,
        (sds((WIDTH, FF), F32), sds((WIDTH, FF), F32), sds((FF, WIDTH), F32), rows_type),
        (
            x0, x1, x2, xt3, xb3, y0, t1, b1, t2, b2, t3, b3, hidden, gate_up, wg, wu,
        ),
        flops=1.9e9,
    )
    grad_gate, grad_up, grad_down = grads
    total = run(sum_kernel, rows_type, (p_own, tl, tr, bl, br), flops=1e6)
    back = exchange(total)
    mid = run(
        combine_kernel,
        sds((TOK, QUART), BF),
        (back, pick, out_cot),
        in_specs=[None, None, quarter_block()],
        flops=7e7,
    )
    m_far = lax.ppermute(mid, "tp", across)
    m_left = lax.ppermute(mid, "tp", to_right)
    m_right = lax.ppermute(mid, "tp", to_left)
    mids = (mid, m_left, m_right, m_far)
    head, pay = run(
        head_kernel,
        (sds((TOK, DV), F32), sds((SLOTS, 2 * LANES), BF)),
        (*mids, w_out, q_dec, state_tile),
        flops=2e8,
    )
    pulled = exchange(pay)
    keep, give = run(out_proj_kernel, (sds((1024, DV), BF),) * 2, (*mids, mixed_heads), flops=1.4e8)
    got = lax.ppermute(give, "sp", other_core)
    tiles = run(split_kernel, (tile_type,) * 4, (keep, got), flops=1e6)
    adds = [lax.ppermute(tiles[k], "sp", along_y(k)) for k in (2, 1, 3)]
    pay = run(
        scan_kernel,
        sds((SLOTS, 2 * LANES), BF),
        (pulled, tiles[0], *adds),
        flops=1e8,
        scratch=[pltpu.VMEM((SLOTS, LANES), F32)] * 3,
    )
    back_states = exchange(pay)
    d_in = run(
        inside_kernel,
        (sds((TOK, DK), F32), sds((TOK, DK), F32), sds((TOK, DV), F32)),
        (keys, values, cum, q_dec, head),
        flops=3e8,
    )
    grad_queries, grad_keys, grad_values, grad_decay, grad_out_proj = run(
        last_kernel,
        (
            sds((TOK, DK), BF),
            sds((TOK, DK), BF),
            sds((TOK, DV), BF),
            sds((TOK, DK), F32),
            sds((32, DV), F32),
        ),
        (keys, values, cum, q_dec, head, *d_in, back_states),
        flops=3e8,
    )
    return (
        grad_gate[None],
        grad_up[None],
        grad_down[None],
        grad_out_proj,
        grad_queries,
        grad_keys,
        grad_values,
        grad_decay,
    )


def solution(mesh):
    return jax.shard_map(
        per_device,
        mesh=mesh,
        in_specs=(
            P("sp", None),
            P("sp", None),
            P("sp", None),
            P("sp", None),
            P("sp", None, "tp"),
            P("sp", None, "tp"),
            P("sp", "tp", None),
            P(None, "tp"),
            P("sp", "tp"),
            P("sp", "tp"),
            P("sp", "tp"),
            P("sp", "tp"),
            P("sp", "tp"),
        ),
        out_specs=(
            P("sp", None, "tp"),
            P("sp", None, "tp"),
            P("sp", "tp", None),
            P("sp", "tp"),
            P("sp", "tp"),
            P("sp", "tp"),
            P("sp", "tp"),
            P("sp", "tp"),
        ),
        check_vma=False,
    )
```

```python
import functools

import jax
import jax.numpy as jnp
from jax import lax
from jax.experimental import pallas as pl
from jax.experimental.pallas import tpu as pltpu
from jax.sharding import PartitionSpec as P


BF = jnp.bfloat16
F32 = jnp.float32
HI = lax.Precision.HIGHEST

TOK = 128
EXPERTS = 64
CAP = 8
SLOTS = EXPERTS * CAP
SIDE = SLOTS // 2
CHIPS = EXPERTS // 2
WIDTH = 2048
QUART = 512
FF = 256
DK = 128
DV = 256
LANES = 128
HALF = 64


def dot(a, b, ca, cb, precision=None):
    return lax.dot_general(
        a, b, (((ca,), (cb,)), ((), ())), preferred_element_type=F32, precision=precision
    )


def iota(shape, dim):
    return lax.broadcasted_iota(jnp.int32, shape, dim)


def rounded(x):
    return x.astype(BF).astype(F32)


def lower_lanes(shape):
    return iota(shape, len(shape) - 1) < HALF


def call(kernel, out_shape, args, *, index, in_specs=None, flops=0, vmem=24, scratch=()):
    nbytes = sum(a.size * a.dtype.itemsize for a in args)
    nbytes += sum(o.size * o.dtype.itemsize for o in jax.tree.leaves(out_shape))

    def whole(a):
        rank = len(a.shape)
        return pl.BlockSpec(a.shape, lambda i, q: (0,) * rank)

    specs = [whole(a) if s is None else s for a, s in zip(args, in_specs or [None] * len(args))]
    return pl.pallas_call(
        kernel,
        out_shape=out_shape,
        grid_spec=pltpu.PrefetchScalarGridSpec(
            num_scalar_prefetch=1,
            grid=(1,),
            in_specs=specs,
            out_specs=jax.tree.map(whole, out_shape),
            scratch_shapes=scratch,
        ),
        compiler_params=pltpu.CompilerParams(vmem_limit_bytes=vmem * 2**20),
        cost_estimate=pl.CostEstimate(
            flops=int(flops), bytes_accessed=int(nbytes), transcendentals=0
        ),
    )(index, *args)


def in_hbm(a):
    return pltpu.with_memory_space_constraint(a, pltpu.HBM)


def sds(shape, dtype):
    return jax.ShapeDtypeStruct(shape, dtype)


def quarter_rows(q):
    return pl.ds(pl.multiple_of(q * QUART, QUART), QUART)


def cumulative_sum(g):
    lower = (iota((TOK, TOK), 0) >= iota((TOK, TOK), 1)).astype(F32)
    return dot(lower, g, 1, 0, HI)


def tiles_of(state, fill=None):
    out = []
    for b in range(4):
        t = state[:, LANES * (b // 2) : LANES * (b // 2 + 1)]
        r = pltpu.roll(t, HALF, 1)
        low, up = (t, r) if b % 2 == 0 else (r, t)
        upper = fill if fill is not None else up - rounded(up)
        tile = jnp.where(lower_lanes(t.shape), rounded(low), upper)
        out.append(tile.reshape(16, 8, LANES))
    return jnp.concatenate(out, axis=1).reshape(SLOTS, LANES)


def state_of(tiles, upper):
    other = pltpu.roll(tiles, HALF, 1)
    even, odd = (other, tiles) if upper else (tiles, other)
    even, odd = even.reshape(16, 32, LANES), odd.reshape(16, 32, LANES)
    low = lower_lanes((DK, LANES))
    halves = []
    for b in (0, 2):
        first = even[:, 8 * b : 8 * b + 8, :].reshape(DK, LANES)
        second = odd[:, 8 * b + 8 : 8 * b + 16, :].reshape(DK, LANES)
        halves.append(jnp.where(low, first, second))
    return jnp.concatenate(halves, axis=1)


def pick_kernel(ids_ref, x_ref, keep_ref, give_ref, pick_ref, slot_ref, own_ref, sem):
    start = pl.multiple_of(lax.axis_index("tp") * QUART, QUART)
    copy = pltpu.make_async_copy(x_ref.at[:, pl.ds(start, QUART)], own_ref, sem)
    copy.start()
    core = lax.rem(lax.axis_index("sp"), 2)
    expert = iota((EXPERTS, TOK), 0)
    id0, id1 = ids_ref[0:1, :], ids_ref[1:2, :]
    hit0, hit1 = expert == id0, expert == id1
    named = (hit0.astype(F32) + hit1.astype(F32)).astype(BF)
    before = (iota((TOK, TOK), 0) < iota((TOK, TOK), 1)).astype(F32).astype(BF)
    count = dot(named, before, 1, 0)
    rank0 = jnp.sum(jnp.where(hit0, count, 0.0), axis=0, keepdims=True)
    rank1 = jnp.sum(jnp.where(hit1, count, 0.0), axis=0, keepdims=True)

    def slot_of(expert_id, rank):
        side = jnp.bitwise_xor(jnp.bitwise_and(expert_id, 1), core)
        return side * SIDE + (expert_id // 2) * CAP + rank.astype(jnp.int32)

    slot0, slot1 = slot_of(id0, rank0), slot_of(id1, rank1)
    slot_ref[0:1, :] = slot0
    slot_ref[1:2, :] = slot1
    slot = iota((SLOTS, TOK), 0)
    pick = ((slot == slot0).astype(F32) + (slot == slot1).astype(F32)).astype(BF)
    pick_ref[...] = pick
    copy.wait()
    rows = dot(pick, own_ref[...], 1, 0).astype(BF)
    keep_ref[...] = rows[:SIDE]
    give_ref[...] = rows[SIDE:]


def weave_kernel(q_ref, keep_ref, got_ref, out_ref):
    keep = keep_ref[...].astype(F32).reshape(CHIPS, CAP, QUART)
    got = got_ref[...].astype(F32).reshape(CHIPS, CAP, QUART)
    out_ref[...] = jnp.concatenate([keep, got], axis=1).reshape(SLOTS, QUART).astype(BF)


def local_kernel(
    q_ref, slot_ref, w_ref, pick_ref, oc_ref, qry_ref, k_ref, v_ref, g_ref,
    keep_ref, give_ref, tile_ref, cum_ref, dec_ref,
):
    slot = iota((SLOTS, TOK), 0)
    at0, at1 = slot == slot_ref[0:1, :], slot == slot_ref[1:2, :]
    weight = jnp.sum(
        jnp.where(at0, w_ref[0:1, :], 0.0) + jnp.where(at1, w_ref[1:2, :], 0.0),
        axis=1,
        keepdims=True,
    )
    rows = (dot(pick_ref[...], oc_ref[...], 1, 0) * weight).astype(BF)
    keep_ref[...] = rows[:SIDE]
    give_ref[...] = rows[SIDE:]
    g = g_ref[...]
    cum = cumulative_sum(g)
    cum_ref[...] = cum
    dec_ref[...] = qry_ref[...].astype(F32) * jnp.exp(cum)
    to_end = k_ref[...].astype(F32) * jnp.exp(cum[TOK - 1 : TOK, :] - cum)
    state = dot(to_end.T, v_ref[...].astype(F32), 1, 0, HI)
    factor = jnp.exp(jnp.sum(g.T, axis=1, keepdims=True))
    high = rounded(factor)
    fill = jnp.where(iota((DK, LANES), 1) < 96, high, factor - high)
    tile_ref[...] = tiles_of(state, fill).astype(BF)


def gate_near_kernel(q_ref, x0_ref, x1_ref, x2_ref, wg_ref, wu_ref, g_ref, u_ref):
    g = u = None
    for n, ref in enumerate((x0_ref, x1_ref, x2_ref)):
        rows = quarter_rows(q_ref[n])
        x = ref[...]
        g1, u1 = dot(x, wg_ref[rows, :], 1, 0), dot(x, wu_ref[rows, :], 1, 0)
        g, u = (g1, u1) if g is None else (g + g1, u + u1)
    g_ref[...] = g
    u_ref[...] = u


def gate_far_kernel(
    q_ref, g_ref, u_ref, t3_ref, b3_ref, wg_ref, wu_ref, hid_ref, to_gate_ref, to_up_ref
):
    rows = quarter_rows(q_ref[3])
    x = jnp.concatenate([t3_ref[...], b3_ref[...]], axis=0)
    g = g_ref[...] + dot(x, wg_ref[rows, :], 1, 0)
    u = u_ref[...] + dot(x, wu_ref[rows, :], 1, 0)
    sig = jax.nn.sigmoid(g)
    silu = g * sig
    hid_ref[...] = (silu * u).astype(BF)
    to_gate_ref[...] = u * sig * (1.0 + g * (1.0 - sig))
    to_up_ref[...] = silu


TOP, BOTTOM = slice(0, SLOTS // 2), slice(SLOTS // 2, SLOTS)


def near_kernel(q_ref, y0_ref, t1_ref, b1_ref, t2_ref, b2_ref, wd_ref, h_ref):
    w0, w1, w2 = (wd_ref[:, quarter_rows(q_ref[n])] for n in range(3))
    h = dot(y0_ref[...], w0, 1, 1)
    h_ref[TOP, :] = h[TOP] + dot(t1_ref[...], w1, 1, 1) + dot(t2_ref[...], w2, 1, 1)
    h_ref[BOTTOM, :] = h[BOTTOM] + dot(b1_ref[...], w1, 1, 1) + dot(b2_ref[...], w2, 1, 1)


def back_rows(gu_ref, wg_ref, wu_ref, rows):
    part = dot(gu_ref[:, :FF], wg_ref[rows, :], 1, 1) + dot(gu_ref[:, FF:], wu_ref[rows, :], 1, 1)
    return part.astype(BF)


def far_kernel(
    q_ref, h_ref, t3_ref, b3_ref, to_gate_ref, to_up_ref, wg_ref, wu_ref, wd_ref,
    gu_ref, top_ref, bottom_ref,
):
    w3 = wd_ref[:, quarter_rows(q_ref[3])]
    for rows, ref in ((TOP, t3_ref), (BOTTOM, b3_ref)):
        h = h_ref[rows, :] + dot(ref[...], w3, 1, 1)
        gu_ref[rows, :FF] = (h * to_gate_ref[rows, :]).astype(BF)
        gu_ref[rows, FF:] = (h * to_up_ref[rows, :]).astype(BF)
    far = back_rows(gu_ref, wg_ref, wu_ref, quarter_rows(q_ref[3]))
    top_ref[...] = far[TOP]
    bottom_ref[...] = far[BOTTOM]


def sides_kernel(q_ref, gu_ref, wg_ref, wu_ref, rt_ref, rb_ref, lt_ref, lb_ref):
    for n, top_ref, bottom_ref in ((2, rt_ref, rb_ref), (1, lt_ref, lb_ref)):
        part = back_rows(gu_ref, wg_ref, wu_ref, quarter_rows(q_ref[n]))
        top_ref[...] = part[TOP]
        bottom_ref[...] = part[BOTTOM]


def merge_kernel(q_ref, rt_ref, lb_ref, from_left_ref, from_right_ref, t_ref, b_ref):
    t_ref[...] = (rt_ref[...].astype(F32) + from_left_ref[...].astype(F32)).astype(BF)
    b_ref[...] = (lb_ref[...].astype(F32) + from_right_ref[...].astype(F32)).astype(BF)


def down_kernel(
    q_ref, y0_ref, t1_ref, b1_ref, t2_ref, b2_ref, t3_ref, b3_ref, hid_ref, gu_ref, wg_ref, wu_ref,
    gd_ref, own_ref,
):
    own_ref[...] = back_rows(gu_ref, wg_ref, wu_ref, quarter_rows(q_ref[0]))
    hid_t = hid_ref[...].T
    pairs = ((t1_ref, b1_ref), (t2_ref, b2_ref), (t3_ref, b3_ref))
    cots = [y0_ref[...]] + [jnp.concatenate([t[...], b[...]], axis=0) for t, b in pairs]
    for n, dy in enumerate(cots):
        gd_ref[:, quarter_rows(q_ref[n])] = dot(hid_t, dy, 1, 0)


def weight_kernel(
    q_ref, x0_ref, x1_ref, x2_ref, xt_ref, xb_ref, gu_ref, gg_ref, gup_ref
):
    gu = gu_ref[...]
    far = jnp.concatenate([xt_ref[...], xb_ref[...]], axis=0)
    for n, x in enumerate((x0_ref[...], x1_ref[...], x2_ref[...], far)):
        rows = quarter_rows(q_ref[n])
        both = dot(x.T, gu, 1, 0)
        gg_ref[rows, :] = both[:, :FF]
        gup_ref[rows, :] = both[:, FF:]


def sum_kernel(q_ref, own_ref, tl_ref, tr_ref, bl_ref, br_ref, out_ref):
    for rows, a_ref, b_ref in ((TOP, tl_ref, tr_ref), (BOTTOM, bl_ref, br_ref)):
        got = a_ref[...].astype(F32) + b_ref[...].astype(F32)
        out_ref[rows, :] = (own_ref[rows, :].astype(F32) + got).astype(BF)


def combine_kernel(q_ref, rows_ref, got_ref, pick_ref, oc_ref, out_ref):
    keep = rows_ref[...].astype(F32).reshape(CHIPS, 2 * CAP, QUART)[:, :CAP, :]
    keep = keep.reshape(SIDE, QUART).astype(BF)
    pick = pick_ref[...].T
    routed = dot(pick[:, :SIDE], keep, 1, 0) + dot(pick[:, SIDE:], got_ref[...], 1, 0)
    out_ref[...] = (oc_ref[...].astype(F32) + routed).astype(BF)


def head_kernel(
    q_ref, m0_ref, m1_ref, m2_ref, m3_ref, w_ref, dec_ref, tile_ref, h_ref, pay_ref
):
    head = None
    for n, ref in enumerate((m0_ref, m1_ref, m2_ref, m3_ref)):
        part = dot(ref[...], w_ref[quarter_rows(q_ref[n]), :], 1, 0)
        head = part if head is None else head + part
    h_ref[...] = head
    pay_ref[:, :LANES] = tiles_of(dot(dec_ref[...].T, head, 1, 0, HI)).astype(BF)
    pay_ref[:, LANES:] = tile_ref[...]


def out_proj_kernel(q_ref, m0_ref, m1_ref, m2_ref, m3_ref, mixed_ref, keep_ref, give_ref):
    mixed = mixed_ref[...]
    first = q_ref[4] == 0
    for n, ref in enumerate((m0_ref, m1_ref, m2_ref, m3_ref)):
        part = dot(ref[...].T, mixed, 1, 0).reshape(16, 32, DV)
        low = part[:, :16, :].reshape(256, DV)
        high = part[:, 16:, :].reshape(256, DV)
        rows = pl.ds(pl.multiple_of(q_ref[n] * 256, 256), 256)
        keep_ref[rows, :] = jnp.where(first, low, high).astype(BF)
        give_ref[rows, :] = jnp.where(first, high, low).astype(BF)


def split_kernel(q_ref, keep_ref, got_ref, o0_ref, o1_ref, o2_ref, o3_ref):
    total = (keep_ref[...].astype(F32) + got_ref[...].astype(F32)).reshape(64, 16, DV)
    tile = [
        total[:, 8 * (n // 2) : 8 * (n // 2) + 8, LANES * (n % 2) : LANES * (n % 2) + LANES]
        for n in range(4)
    ]
    tile = [t.reshape(SLOTS, LANES) for t in tile]
    y = q_ref[5]
    for k, ref in enumerate((o0_ref, o1_ref, o2_ref, o3_ref)):
        out = tile[k]
        for n in range(1, 4):
            out = jnp.where(y == n, tile[(n + k) % 4], out)
        ref[...] = out.astype(BF)


def scan_kernel(
    q_ref, in_ref, o_ref, r1_ref, r2_ref, r3_ref, out_ref, factor_ref, pre_ref, suf_ref
):
    pull = in_ref[:, :LANES].astype(F32)
    suf_ref[...] = pull + pltpu.roll(pull, HALF, 1)
    tile = in_ref[:, LANES:].astype(F32)
    pre_ref[...] = pltpu.roll(tile, HALF, 1)
    factor_ref[...] = jnp.broadcast_to(tile[:, 64:65] + tile[:, 96:97], tile.shape)
    before = after = jnp.zeros((8, LANES), F32)
    for s in range(EXPERTS):
        rows = slice(8 * s, 8 * s + 8)
        now = pre_ref[rows, :]
        pre_ref[rows, :] = before
        before = before * factor_ref[rows, :] + now
        e = EXPERTS - 1 - s
        rows = slice(8 * e, 8 * e + 8)
        now = suf_ref[rows, :]
        suf_ref[rows, :] = after
        after = after * factor_ref[rows, :] + now
    suf = suf_ref[...]
    out_ref[:, :LANES] = jnp.where(lower_lanes(suf.shape), suf, pre_ref[...]).astype(BF)
    total = o_ref[...].astype(F32) + r1_ref[...].astype(F32)
    out_ref[:, LANES:] = (total + r2_ref[...].astype(F32) + r3_ref[...].astype(F32)).astype(BF)


def inside_kernel(
    q_ref, k_ref, v_ref, cum_ref, dec_ref, h_ref, dq_ref, dk_ref, dv_ref
):
    k, v, q_dec, head = k_ref[...].astype(F32), v_ref[...].astype(F32), dec_ref[...], h_ref[...]
    k_grown = k * jnp.exp(-cum_ref[...])
    causal = iota((TOK, TOK), 0) >= iota((TOK, TOK), 1)
    score = jnp.where(causal, dot(q_dec, k_grown, 1, 1, HI), 0.0)
    d_score = jnp.where(causal, dot(head, v, 1, 1, HI), 0.0)
    dq_ref[...] = dot(d_score, k_grown, 1, 0, HI)
    dk_ref[...] = dot(d_score.T, q_dec, 1, 0, HI)
    dv_ref[...] = dot(score.T, head, 1, 0, HI)


def last_kernel(
    q_ref, k_ref, v_ref, cum_ref, dec_ref, h_ref, dq_ref, dk_ref, dv_ref, in_ref,
    gq_ref, gk_ref, gv_ref, gg_ref, go_ref,
):
    tiles = in_ref[:, :LANES].astype(F32)
    cot, state = state_of(tiles, False), state_of(tiles, True)
    k, v, head, cum = k_ref[...].astype(F32), v_ref[...].astype(F32), h_ref[...], cum_ref[...]
    last = cum[TOK - 1 : TOK, :]
    shrink, to_end = jnp.exp(-cum), jnp.exp(last - cum)
    k_end = k * to_end
    d_q = dq_ref[...] + dot(head, state, 1, 1, HI)
    d_kg = dk_ref[...]
    d_ke = dot(v, cot, 1, 1, HI)
    gq_ref[...] = (d_q * jnp.exp(cum)).astype(BF)
    gk_ref[...] = (d_kg * shrink + d_ke * to_end).astype(BF)
    gv_ref[...] = (dv_ref[...] + dot(k_end, cot, 1, 0, HI)).astype(BF)
    end = d_ke * k_end
    d_cum = d_q * dec_ref[...] - d_kg * (k * shrink) - end
    carried = jnp.sum((state * cot).T, axis=0, keepdims=True)
    d_last = jnp.sum(end, axis=0, keepdims=True) + jnp.exp(last) * carried
    upper = (iota((TOK, TOK), 0) <= iota((TOK, TOK), 1)).astype(F32)
    gg_ref[...] = dot(upper, d_cum, 1, 0, HI) + d_last
    parts = jnp.sum(in_ref[:, LANES:].astype(F32).reshape(8, EXPERTS, LANES), axis=0)
    for y in range(4):
        for core in range(2):
            n = 8 * (2 * y + core)
            rows = 16 * core + 8 * (y // 2)
            lanes = LANES * (y % 2)
            go_ref[rows : rows + 8, lanes : lanes + LANES] = parts[n : n + 8, :]


def per_device(
    expert_in, out_cot, route_ids, route_weights, w_gate, w_up, w_down, w_out,
    mixed_heads, queries, keys, values, log_decay,
):
    me, sp = lax.axis_index("tp"), lax.axis_index("sp")
    table = [
        [i, (i + 3) % 4, (i + 1) % 4, (i + 2) % 4, s % 2, s // 2] for s in range(8) for i in range(4)
    ]
    place = lax.rem(sp, 8) * 4 + me
    order = lax.dynamic_slice(jnp.array(table, jnp.int32).reshape(-1), (place * 6,), (6,))
    to_right = [(i, (i + 1) % 4) for i in range(4)]
    to_left = [(i, (i + 3) % 4) for i in range(4)]
    across = [(i, (i + 2) % 4) for i in range(4)]
    other_core = [(i, i ^ 1) for i in range(64)]

    def along_y(k):
        return [(i, i // 8 * 8 + (i + 2 * k) % 8) for i in range(64)]

    wg, wu, wd = w_gate[0], w_up[0], w_down[0]
    run = functools.partial(call, index=order)

    def exchange(rows):
        width = rows.shape[1]
        got = lax.all_to_all(rows.reshape(EXPERTS, CAP, width), "sp", 0, 0, tiled=True)
        return got.reshape(SLOTS, width)

    def quarter_block():
        return pl.BlockSpec((TOK, QUART), lambda i, q: (0, q[0]))

    rows_type = sds((SLOTS, QUART), BF)
    tile_type = sds((SLOTS, LANES), BF)
    side_type = sds((SIDE, QUART), BF)

    def between_chips(rows):
        groups = [list(range(core, 64, 2)) for core in range(2)]
        got = lax.all_to_all(
            rows.reshape(CHIPS, 2 * CAP, QUART), "sp", 0, 0, tiled=True, axis_index_groups=groups
        )
        return got.reshape(SLOTS, QUART)

    x_keep, x_give, pick, slots = pl.pallas_call(
        pick_kernel,
        out_shape=(side_type, side_type, sds((SLOTS, TOK), BF), sds((2, TOK), jnp.int32)),
        in_specs=[
            pl.BlockSpec(memory_space=pltpu.VMEM),
            pl.BlockSpec(memory_space=pltpu.HBM),
        ],
        out_specs=(pl.BlockSpec(memory_space=pltpu.VMEM),) * 4,
        scratch_shapes=[pltpu.VMEM((TOK, QUART), BF), pltpu.SemaphoreType.DMA],
        compiler_params=pltpu.CompilerParams(vmem_limit_bytes=24 * 2**20),
        cost_estimate=pl.CostEstimate(
            flops=10**8, bytes_accessed=2 * 10**6, transcendentals=0
        ),
    )(in_hbm(route_ids.T), expert_in)
    x_got = lax.ppermute(x_give, "sp", other_core)
    x_rows = run(weave_kernel, rows_type, (x_keep, x_got), flops=1e6)
    y_keep, y_give, state_tile, cum, q_dec = run(
        local_kernel,
        (side_type, side_type, tile_type, sds((TOK, DK), F32), sds((TOK, DK), F32)),
        (
            slots, in_hbm(route_weights.T), pick, in_hbm(out_cot), in_hbm(queries), in_hbm(keys),
            in_hbm(values), in_hbm(log_decay),
        ),
        in_specs=[None, None, None, quarter_block(), None, None, None, None],
        flops=3e8,
    )
    y_got = lax.ppermute(y_give, "sp", other_core)
    y_rows = run(weave_kernel, rows_type, (y_keep, y_got), flops=1e6)
    x0 = between_chips(x_rows)
    x0, y_rows = lax.optimization_barrier((x0, y_rows))
    x1 = lax.ppermute(x0, "tp", to_right)
    x2 = lax.ppermute(x0, "tp", to_left)
    xt3 = lax.ppermute(x1[TOP], "tp", to_right)
    xb3 = lax.ppermute(x2[BOTTOM], "tp", to_left)
    y0 = between_chips(y_rows)
    y_top, y_bottom = y0[TOP], y0[BOTTOM]
    t1 = lax.ppermute(y_top, "tp", to_right)
    b2 = lax.ppermute(y_bottom, "tp", to_left)
    b1 = lax.ppermute(y_bottom, "tp", to_right)
    t2 = lax.ppermute(y_top, "tp", to_left)
    t3 = lax.ppermute(t1, "tp", to_right)
    b3 = lax.ppermute(b2, "tp", to_left)
    half_type = sds((SLOTS, FF), F32)
    part_type = sds((SLOTS // 2, QUART), BF)
    g, u = run(gate_near_kernel, (half_type,) * 2, (x0, x1, x2, wg, wu), flops=8e8)
    hidden, to_gate, to_up = run(
        gate_far_kernel,
        (sds((SLOTS, FF), BF), half_type, half_type),
        (g, u, xt3, xb3, wg, wu),
        flops=3e8,
    )
    h = run(near_kernel, half_type, (y0, t1, b1, t2, b2, wd), flops=4e8)
    gate_up, p_top, p_bottom = run(
        far_kernel,
        (sds((SLOTS, 2 * FF), BF), part_type, part_type),
        (h, t3, b3, to_gate, to_up, wg, wu, wd),
        flops=4e8,
    )
    far_top = lax.ppermute(p_top, "tp", to_right)
    far_bottom = lax.ppermute(p_bottom, "tp", to_left)
    p_rt, p_rb, p_lt, p_lb = run(sides_kernel, (part_type,) * 4, (gate_up, wg, wu), flops=5e8)
    bl = lax.ppermute(p_rb, "tp", to_right)
    tr = lax.ppermute(p_lt, "tp", to_left)
    grad_down, p_own = run(
        down_kernel,
        (sds((FF, WIDTH), F32), rows_type),
        (y0, t1, b1, t2, b2, t3, b3, hidden, gate_up, wg, wu),
        flops=8e8,
    )
    far_top, p_own = lax.optimization_barrier((far_top, p_own))
    p_t, p_b = run(merge_kernel, (part_type,) * 2, (p_rt, p_lb, far_top, far_bottom), flops=1e6)
    tl = lax.ppermute(p_t, "tp", to_right)
    br = lax.ppermute(p_b, "tp", to_left)
    grads = run(
        weight_kernel,
        (sds((WIDTH, FF), F32), sds((WIDTH, FF), F32)),
        (x0, x1, x2, xt3, xb3, gate_up),
        flops=1.1e9,
    )
    p_own, grads = lax.optimization_barrier((p_own, grads))
    grad_gate, grad_up = grads
    total = run(sum_kernel, rows_type, (p_own, tl, tr, bl, br), flops=1e6)
    back = between_chips(total)
    give = back.reshape(CHIPS, 2 * CAP, QUART)[:, CAP:, :].reshape(SIDE, QUART)
    got = lax.ppermute(give, "sp", other_core)
    mid = run(
        combine_kernel,
        sds((TOK, QUART), BF),
        (back, got, pick, out_cot),
        in_specs=[None, None, None, quarter_block()],
        flops=7e7,
    )
    m_far = lax.ppermute(mid, "tp", across)
    m_left = lax.ppermute(mid, "tp", to_right)
    m_right = lax.ppermute(mid, "tp", to_left)
    mids = (mid, m_left, m_right, m_far)
    head, pay = run(
        head_kernel,
        (sds((TOK, DV), F32), sds((SLOTS, 2 * LANES), BF)),
        (*mids, w_out, q_dec, state_tile),
        flops=2e8,
    )
    pulled = exchange(pay)
    keep, give = run(out_proj_kernel, (sds((1024, DV), BF),) * 2, (*mids, mixed_heads), flops=1.4e8)
    got = lax.ppermute(give, "sp", other_core)
    tiles = run(split_kernel, (tile_type,) * 4, (keep, got), flops=1e6)
    adds = [lax.ppermute(tiles[k], "sp", along_y(k)) for k in (2, 1, 3)]
    pay = run(
        scan_kernel,
        sds((SLOTS, 2 * LANES), BF),
        (pulled, tiles[0], *adds),
        flops=1e8,
        scratch=[pltpu.VMEM((SLOTS, LANES), F32)] * 3,
    )
    back_states = exchange(pay)
    d_in = run(
        inside_kernel,
        (sds((TOK, DK), F32), sds((TOK, DK), F32), sds((TOK, DV), F32)),
        (keys, values, cum, q_dec, head),
        flops=3e8,
    )
    grad_queries, grad_keys, grad_values, grad_decay, grad_out_proj = run(
        last_kernel,
        (
            sds((TOK, DK), BF),
            sds((TOK, DK), BF),
            sds((TOK, DV), BF),
            sds((TOK, DK), F32),
            sds((32, DV), F32),
        ),
        (keys, values, cum, q_dec, head, *d_in, back_states),
        flops=3e8,
    )
    return (
        grad_gate[None],
        grad_up[None],
        grad_down[None],
        grad_out_proj,
        grad_queries,
        grad_keys,
        grad_values,
        grad_decay,
    )


def solution(mesh):
    return jax.shard_map(
        per_device,
        mesh=mesh,
        in_specs=(
            P("sp", None),
            P("sp", None),
            P("sp", None),
            P("sp", None),
            P("sp", None, "tp"),
            P("sp", None, "tp"),
            P("sp", "tp", None),
            P(None, "tp"),
            P("sp", "tp"),
            P("sp", "tp"),
            P("sp", "tp"),
            P("sp", "tp"),
            P("sp", "tp"),
        ),
        out_specs=(
            P("sp", None, "tp"),
            P("sp", None, "tp"),
            P("sp", "tp", None),
            P("sp", "tp"),
            P("sp", "tp"),
            P("sp", "tp"),
            P("sp", "tp"),
            P("sp", "tp"),
        ),
        check_vma=False,
    )
```

```python
import functools

import jax
import jax.numpy as jnp
from jax import lax
from jax.experimental import pallas as pl
from jax.experimental.pallas import tpu as pltpu
from jax.sharding import PartitionSpec as P


BF = jnp.bfloat16
F32 = jnp.float32
HI = lax.Precision.HIGHEST

TOK = 128
EXPERTS = 64
CAP = 8
SLOTS = EXPERTS * CAP
SIDE = SLOTS // 2
CHIPS = EXPERTS // 2
WIDTH = 2048
QUART = 512
FF = 256
DK = 128
DV = 256
LANES = 128
HALF = 64


def dot(a, b, ca, cb, precision=None):
    return lax.dot_general(
        a, b, (((ca,), (cb,)), ((), ())), preferred_element_type=F32, precision=precision
    )


def iota(shape, dim):
    return lax.broadcasted_iota(jnp.int32, shape, dim)


def rounded(x):
    return x.astype(BF).astype(F32)


def call(kernel, out_shape, args, *, index, in_specs=None, flops=0, vmem=24, scratch=()):
    nbytes = sum(a.size * a.dtype.itemsize for a in args)
    nbytes += sum(o.size * o.dtype.itemsize for o in jax.tree.leaves(out_shape))

    def whole(a):
        rank = len(a.shape)
        return pl.BlockSpec(a.shape, lambda i, q: (0,) * rank)

    specs = [whole(a) if s is None else s for a, s in zip(args, in_specs or [None] * len(args))]
    return pl.pallas_call(
        kernel,
        out_shape=out_shape,
        grid_spec=pltpu.PrefetchScalarGridSpec(
            num_scalar_prefetch=1,
            grid=(1,),
            in_specs=specs,
            out_specs=jax.tree.map(whole, out_shape),
            scratch_shapes=scratch,
        ),
        compiler_params=pltpu.CompilerParams(vmem_limit_bytes=vmem * 2**20),
        cost_estimate=pl.CostEstimate(
            flops=int(flops), bytes_accessed=int(nbytes), transcendentals=0
        ),
    )(index, *args)


def in_hbm(a):
    return pltpu.with_memory_space_constraint(a, pltpu.HBM)


def sds(shape, dtype):
    return jax.ShapeDtypeStruct(shape, dtype)


def quarter_rows(q):
    return pl.ds(pl.multiple_of(q * QUART, QUART), QUART)


def cumulative_sum(g):
    lower = (iota((TOK, TOK), 0) >= iota((TOK, TOK), 1)).astype(F32)
    return dot(lower, g, 1, 0, HI)


def dot_rounded(a, b, ca, cb):
    high = a.astype(BF)
    return dot(high, b, ca, cb) + dot((a - high.astype(F32)).astype(BF), b, ca, cb)


def pick_kernel(
    ids_hbm, x_ref, keep_ref, give_ref, pick_ref, slot_ref, ids_ref, own_ref, ids_sem, sem
):
    ids_copy = pltpu.make_async_copy(ids_hbm, ids_ref, ids_sem)
    ids_copy.start()
    start = pl.multiple_of(lax.axis_index("tp") * QUART, QUART)
    copy = pltpu.make_async_copy(x_ref.at[:, pl.ds(start, QUART)], own_ref, sem)
    copy.start()
    core = lax.rem(lax.axis_index("sp"), 2)
    expert = iota((EXPERTS, TOK), 0)
    ids_copy.wait()
    id0, id1 = ids_ref[0:1, :], ids_ref[1:2, :]
    hit0, hit1 = expert == id0, expert == id1
    named = (hit0.astype(F32) + hit1.astype(F32)).astype(BF)
    before = (iota((TOK, TOK), 0) < iota((TOK, TOK), 1)).astype(F32).astype(BF)
    count = dot(named, before, 1, 0)
    rank0 = jnp.sum(jnp.where(hit0, count, 0.0), axis=0, keepdims=True)
    rank1 = jnp.sum(jnp.where(hit1, count, 0.0), axis=0, keepdims=True)

    def slot_of(expert_id, rank):
        side = jnp.bitwise_xor(jnp.bitwise_and(expert_id, 1), core)
        return side * SIDE + (expert_id // 2) * CAP + rank.astype(jnp.int32)

    slot0, slot1 = slot_of(id0, rank0), slot_of(id1, rank1)
    slot_ref[0:1, :] = slot0
    slot_ref[1:2, :] = slot1
    slot = iota((SLOTS, TOK), 0)
    pick = ((slot == slot0).astype(F32) + (slot == slot1).astype(F32)).astype(BF)
    pick_ref[...] = pick
    copy.wait()
    rows = dot(pick, own_ref[...], 1, 0).astype(BF)
    keep_ref[...] = rows[:SIDE]
    give_ref[...] = rows[SIDE:]


def weave_kernel(q_ref, keep_ref, got_ref, out_ref):
    keep = keep_ref[...].astype(F32).reshape(CHIPS, CAP, QUART)
    got = got_ref[...].astype(F32).reshape(CHIPS, CAP, QUART)
    out_ref[...] = jnp.concatenate([keep, got], axis=1).reshape(SLOTS, QUART).astype(BF)


def local_kernel(
    q_ref, slot_ref, w_ref, pick_ref, oc_ref, qry_ref, k_ref, v_ref, g_ref,
    keep_ref, give_ref, tile_ref, cum_ref, dec_ref,
):
    slot = iota((SLOTS, TOK), 0)
    at0, at1 = slot == slot_ref[0:1, :], slot == slot_ref[1:2, :]
    weight = jnp.sum(
        jnp.where(at0, w_ref[0:1, :], 0.0) + jnp.where(at1, w_ref[1:2, :], 0.0),
        axis=1,
        keepdims=True,
    )
    rows = (dot(pick_ref[...], oc_ref[...], 1, 0) * weight).astype(BF)
    keep_ref[...] = rows[:SIDE]
    give_ref[...] = rows[SIDE:]
    g = g_ref[...]
    cum = cumulative_sum(g)
    cum_ref[...] = cum
    dec_ref[...] = qry_ref[...].astype(F32) * jnp.exp(cum)
    to_end = k_ref[...].astype(F32) * jnp.exp(cum[TOK - 1 : TOK, :] - cum)
    state = dot(to_end.T, v_ref[...].astype(F32), 1, 0, HI)
    factor = jnp.exp(jnp.sum(g.T, axis=1, keepdims=True))
    high = rounded(factor)
    tile_ref[:, :DV] = state.astype(BF)
    tile_ref[:, DV:] = jnp.where(iota((DK, LANES), 1) < HALF, high, factor - high).astype(BF)


def gate_near_kernel(q_ref, x0_ref, x1_ref, x2_ref, wg_ref, wu_ref, g_ref, u_ref):
    g = u = None
    for n, ref in enumerate((x0_ref, x1_ref, x2_ref)):
        rows = quarter_rows(q_ref[n])
        x = ref[...]
        g1, u1 = dot(x, wg_ref[rows, :], 1, 0), dot(x, wu_ref[rows, :], 1, 0)
        g, u = (g1, u1) if g is None else (g + g1, u + u1)
    g_ref[...] = g
    u_ref[...] = u


def gate_far_kernel(
    q_ref, g_ref, u_ref, t3_ref, b3_ref, wg_ref, wu_ref, hid_ref, to_gate_ref, to_up_ref
):
    rows = quarter_rows(q_ref[3])
    x = jnp.concatenate([t3_ref[...], b3_ref[...]], axis=0)
    g = g_ref[...] + dot(x, wg_ref[rows, :], 1, 0)
    u = u_ref[...] + dot(x, wu_ref[rows, :], 1, 0)
    sig = jax.nn.sigmoid(g)
    silu = g * sig
    hid_ref[...] = (silu * u).astype(BF)
    to_gate_ref[...] = u * sig * (1.0 + g * (1.0 - sig))
    to_up_ref[...] = silu


TOP, BOTTOM = slice(0, SLOTS // 2), slice(SLOTS // 2, SLOTS)


def near_kernel(q_ref, y0_ref, t1_ref, b1_ref, t2_ref, b2_ref, wd_ref, h_ref):
    w0, w1, w2 = (wd_ref[:, quarter_rows(q_ref[n])] for n in range(3))
    h = dot(y0_ref[...], w0, 1, 1)
    h_ref[TOP, :] = h[TOP] + dot(t1_ref[...], w1, 1, 1) + dot(t2_ref[...], w2, 1, 1)
    h_ref[BOTTOM, :] = h[BOTTOM] + dot(b1_ref[...], w1, 1, 1) + dot(b2_ref[...], w2, 1, 1)


def back_rows(gu_ref, wg_ref, wu_ref, rows):
    part = dot(gu_ref[:, :FF], wg_ref[rows, :], 1, 1) + dot(gu_ref[:, FF:], wu_ref[rows, :], 1, 1)
    return part.astype(BF)


def far_kernel(
    q_ref, h_ref, t3_ref, b3_ref, to_gate_ref, to_up_ref, wg_ref, wu_ref, wd_ref,
    gu_ref, top_ref, bottom_ref,
):
    w3 = wd_ref[:, quarter_rows(q_ref[3])]
    for rows, ref in ((TOP, t3_ref), (BOTTOM, b3_ref)):
        h = h_ref[rows, :] + dot(ref[...], w3, 1, 1)
        gu_ref[rows, :FF] = (h * to_gate_ref[rows, :]).astype(BF)
        gu_ref[rows, FF:] = (h * to_up_ref[rows, :]).astype(BF)
    far = back_rows(gu_ref, wg_ref, wu_ref, quarter_rows(q_ref[3]))
    top_ref[...] = far[TOP]
    bottom_ref[...] = far[BOTTOM]


def sides_kernel(q_ref, gu_ref, wg_ref, wu_ref, rt_ref, rb_ref, lt_ref, lb_ref):
    for n, top_ref, bottom_ref in ((2, rt_ref, rb_ref), (1, lt_ref, lb_ref)):
        part = back_rows(gu_ref, wg_ref, wu_ref, quarter_rows(q_ref[n]))
        top_ref[...] = part[TOP]
        bottom_ref[...] = part[BOTTOM]


def merge_kernel(q_ref, rt_ref, lb_ref, from_left_ref, from_right_ref, t_ref, b_ref):
    t_ref[...] = (rt_ref[...].astype(F32) + from_left_ref[...].astype(F32)).astype(BF)
    b_ref[...] = (lb_ref[...].astype(F32) + from_right_ref[...].astype(F32)).astype(BF)


def down_kernel(
    q_ref, y0_ref, t1_ref, b1_ref, t2_ref, b2_ref, t3_ref, b3_ref, hid_ref, gu_ref, wg_ref, wu_ref,
    gd_ref, own_ref,
):
    own_ref[...] = back_rows(gu_ref, wg_ref, wu_ref, quarter_rows(q_ref[0]))
    hid_t = hid_ref[...].T
    pairs = ((t1_ref, b1_ref), (t2_ref, b2_ref), (t3_ref, b3_ref))
    cots = [y0_ref[...]] + [jnp.concatenate([t[...], b[...]], axis=0) for t, b in pairs]
    for n, dy in enumerate(cots):
        gd_ref[:, quarter_rows(q_ref[n])] = dot(hid_t, dy, 1, 0)


def weight_kernel(
    q_ref, x0_ref, x1_ref, x2_ref, xt_ref, xb_ref, gu_ref, gg_ref, gup_ref
):
    gu = gu_ref[...]
    far = jnp.concatenate([xt_ref[...], xb_ref[...]], axis=0)
    for n, x in enumerate((x0_ref[...], x1_ref[...], x2_ref[...], far)):
        rows = quarter_rows(q_ref[n])
        both = dot(x.T, gu, 1, 0)
        gg_ref[rows, :] = both[:, :FF]
        gup_ref[rows, :] = both[:, FF:]


def sum_kernel(q_ref, own_ref, tl_ref, tr_ref, bl_ref, br_ref, out_ref):
    for rows, a_ref, b_ref in ((TOP, tl_ref, tr_ref), (BOTTOM, bl_ref, br_ref)):
        got = a_ref[...].astype(F32) + b_ref[...].astype(F32)
        out_ref[rows, :] = (own_ref[rows, :].astype(F32) + got).astype(BF)


def combine_kernel(q_ref, rows_ref, got_ref, pick_ref, oc_ref, out_ref):
    keep = rows_ref[...].astype(F32).reshape(CHIPS, 2 * CAP, QUART)[:, :CAP, :]
    keep = keep.reshape(SIDE, QUART).astype(BF)
    pick = pick_ref[...].T
    routed = dot(pick[:, :SIDE], keep, 1, 0) + dot(pick[:, SIDE:], got_ref[...], 1, 0)
    out_ref[...] = (oc_ref[...].astype(F32) + routed).astype(BF)


def head_kernel(
    q_ref, m0_ref, m1_ref, m2_ref, m3_ref, w_ref, dec_ref, tile_ref, h_ref, pay_ref
):
    head = None
    for n, ref in enumerate((m0_ref, m1_ref, m2_ref, m3_ref)):
        part = dot(ref[...], w_ref[quarter_rows(q_ref[n]), :], 1, 0)
        head = part if head is None else head + part
    h_ref[...] = head
    pay_ref[:, :DV] = dot(dec_ref[...].T, head, 1, 0, HI).astype(BF)
    pay_ref[:, DV:] = tile_ref[...]


def out_proj_kernel(q_ref, m0_ref, m1_ref, m2_ref, m3_ref, mixed_ref, keep_ref, give_ref):
    mixed = mixed_ref[...]
    first = q_ref[4] == 0
    for n, ref in enumerate((m0_ref, m1_ref, m2_ref, m3_ref)):
        part = dot(ref[...].T, mixed, 1, 0).reshape(8, 64, DV)
        low = part[:, :32, :].reshape(256, DV)
        high = part[:, 32:, :].reshape(256, DV)
        rows = pl.ds(pl.multiple_of(q_ref[n] * 256, 256), 256)
        keep_ref[rows, :] = jnp.where(first, low, high).astype(BF)
        give_ref[rows, :] = jnp.where(first, high, low).astype(BF)


def split_kernel(q_ref, keep_ref, got_ref, o0_ref, o1_ref, o2_ref, o3_ref):
    total = (keep_ref[...].astype(F32) + got_ref[...].astype(F32)).reshape(8, 128, DV)
    slab = []
    for n in range(4):
        block = total[:, 32 * n : 32 * n + 32, :]
        wide = jnp.concatenate([block[:, :16, :], block[:, 16:, :]], axis=2)
        slab.append(wide.reshape(TOK, 2 * DV))
    y = q_ref[5]
    for k, ref in enumerate((o0_ref, o1_ref, o2_ref, o3_ref)):
        out = slab[k]
        for n in range(1, 4):
            out = jnp.where(y == n, slab[(n + k) % 4], out)
        ref[...] = out.astype(BF)


def block_of(n):
    return slice(16 * n, 16 * n + 16)


def factor_of(ref, lane):
    high, low = ref[:, lane : lane + 1], ref[:, lane + HALF : lane + HALF + 1]
    return jnp.broadcast_to(high.astype(F32) + low.astype(F32), (DK, DV))


def plane_kernel(
    q_ref, in_ref, o_ref, r1_ref, r2_ref, r3_ref, pay_ref, suf_ref, pre_ref, factor_ref
):
    factor_ref[...] = factor_of(in_ref, 2 * DV)
    suf = pre = jnp.zeros((16, DV), F32)
    whole = jnp.ones((16, DV), F32)
    for n in range(8):
        rows = block_of(n)
        pre_ref[rows, :] = pre
        pre = pre * factor_ref[rows, :] + in_ref[rows, DV : 2 * DV].astype(F32)
        whole = whole * factor_ref[rows, :]
        rows = block_of(7 - n)
        suf_ref[rows, :] = suf
        suf = suf * factor_ref[rows, :] + in_ref[rows, :DV].astype(F32)
    part = whole[:, :LANES]
    high = rounded(part)
    part = jnp.where(iota(part.shape, 1) < HALF, high, part - high)
    block = jnp.concatenate([suf, pre, part], axis=1)
    pay_ref[:, : 2 * DV + LANES] = jnp.concatenate([block] * 8, axis=0).astype(BF)
    total = o_ref[...].astype(F32) + r1_ref[...].astype(F32)
    total = total + r2_ref[...].astype(F32) + r3_ref[...].astype(F32)
    pay_ref[:, 2 * DV + LANES :] = total.astype(BF)


def line_kernel(
    q_ref, in_ref, suf_ref, pre_ref, factor_ref, pay_ref, go_ref, totals_ref
):
    totals_ref[...] = factor_of(in_ref, 2 * DV)
    z = q_ref[6]
    suf = pre = jnp.zeros((16, DV), F32)
    for n in range(8):
        rows = block_of(n)
        step = pre * totals_ref[rows, :] + in_ref[rows, DV : 2 * DV].astype(F32)
        pre = jnp.where(n < z, step, pre)
        rows = block_of(7 - n)
        step = suf * totals_ref[rows, :] + in_ref[rows, :DV].astype(F32)
        suf = jnp.where(7 - n > z, step, suf)
    for n in range(8):
        rows = block_of(n)
        pay_ref[rows, DV:] = (pre_ref[rows, :] + pre).astype(BF)
        pre = pre * factor_ref[rows, :]
        rows = block_of(7 - n)
        pay_ref[rows, :DV] = (suf_ref[rows, :] + suf).astype(BF)
        suf = suf * factor_ref[rows, :]
    total = jnp.sum(in_ref[:, 2 * DV + LANES :].astype(F32).reshape(8, 16, 2 * DV), axis=0)
    go_ref[:16, :] = total[:, :DV]
    go_ref[16:, :] = total[:, DV:]


def inside_kernel(
    q_ref, k_ref, v_ref, cum_ref, dec_ref, h_ref, dq_ref, dk_ref, dv_ref
):
    k, v, q_dec, head = k_ref[...].astype(F32), v_ref[...].astype(F32), dec_ref[...], h_ref[...]
    k_grown = k * jnp.exp(-cum_ref[...])
    causal = iota((TOK, TOK), 0) >= iota((TOK, TOK), 1)
    score = jnp.where(causal, dot(q_dec, k_grown, 1, 1, HI), 0.0)
    d_score = jnp.where(causal, dot(head, v, 1, 1, HI), 0.0)
    dq_ref[...] = dot(d_score, k_grown, 1, 0, HI)
    dk_ref[...] = dot(d_score.T, q_dec, 1, 0, HI)
    dv_ref[...] = dot(score.T, head, 1, 0, HI)


def last_kernel(
    q_ref, k_ref, v_ref, cum_ref, dec_ref, h_ref, dq_ref, dk_ref, dv_ref, in_ref,
    gq_ref, gk_ref, gv_ref, gg_ref,
):
    cot, state = in_ref[:, :DV], in_ref[:, DV:]
    k, cum = k_ref[...].astype(F32), cum_ref[...]
    last = cum[TOK - 1 : TOK, :]
    shrink, to_end = jnp.exp(-cum), jnp.exp(last - cum)
    k_end = k * to_end
    d_q = dq_ref[...] + dot_rounded(h_ref[...], state, 1, 1)
    d_kg = dk_ref[...]
    d_ke = dot(v_ref[...], cot, 1, 1)
    gq_ref[...] = (d_q * jnp.exp(cum)).astype(BF)
    gk_ref[...] = (d_kg * shrink + d_ke * to_end).astype(BF)
    gv_ref[...] = (dv_ref[...] + dot_rounded(k_end, cot, 1, 0)).astype(BF)
    end = d_ke * k_end
    d_cum = d_q * dec_ref[...] - d_kg * (k * shrink) - end
    carried = jnp.sum((state.astype(F32) * cot.astype(F32)).T, axis=0, keepdims=True)
    d_last = jnp.sum(end, axis=0, keepdims=True) + jnp.exp(last) * carried
    upper = (iota((TOK, TOK), 0) <= iota((TOK, TOK), 1)).astype(F32)
    gg_ref[...] = dot(upper, d_cum, 1, 0, HI) + d_last


def per_device(
    expert_in, out_cot, route_ids, route_weights, w_gate, w_up, w_down, w_out,
    mixed_heads, queries, keys, values, log_decay,
):
    me, sp = lax.axis_index("tp"), lax.axis_index("sp")
    table = [
        [i, (i + 3) % 4, (i + 1) % 4, (i + 2) % 4, s % 2, s // 2 % 4, s // 8]
        for s in range(64)
        for i in range(4)
    ]
    place = (sp * 4 + me) * 7
    order = lax.dynamic_slice(jnp.array(table, jnp.int32).reshape(-1), (place,), (7,))
    to_right = [(i, (i + 1) % 4) for i in range(4)]
    to_left = [(i, (i + 3) % 4) for i in range(4)]
    across = [(i, (i + 2) % 4) for i in range(4)]
    other_core = [(i, i ^ 1) for i in range(64)]

    def along_y(k):
        return [(i, i // 8 * 8 + (i + 2 * k) % 8) for i in range(64)]

    wg, wu, wd = w_gate[0], w_up[0], w_down[0]
    run = functools.partial(call, index=order)

    def exchange(rows, groups):
        width = rows.shape[1]
        got = lax.all_to_all(
            rows.reshape(8, 16, width), "sp", 0, 0, tiled=True, axis_index_groups=groups
        )
        return got.reshape(DK, width)

    in_plane = [[8 * z + n for n in range(8)] for z in range(8)]
    along_z = [[8 * z + n for z in range(8)] for n in range(8)]

    def quarter_block():
        return pl.BlockSpec((TOK, QUART), lambda i, q: (0, q[0]))

    rows_type = sds((SLOTS, QUART), BF)
    tile_type = sds((TOK, 2 * DV), BF)
    side_type = sds((SIDE, QUART), BF)

    def between_chips(rows):
        groups = [list(range(core, 64, 2)) for core in range(2)]
        got = lax.all_to_all(
            rows.reshape(CHIPS, 2 * CAP, QUART), "sp", 0, 0, tiled=True, axis_index_groups=groups
        )
        return got.reshape(SLOTS, QUART)

    x_keep, x_give, pick, slots = pl.pallas_call(
        pick_kernel,
        out_shape=(side_type, side_type, sds((SLOTS, TOK), BF), sds((2, TOK), jnp.int32)),
        in_specs=[pl.BlockSpec(memory_space=pltpu.HBM)] * 2,
        out_specs=(pl.BlockSpec(memory_space=pltpu.VMEM),) * 4,
        scratch_shapes=[
            pltpu.VMEM((2, TOK), jnp.int32),
            pltpu.VMEM((TOK, QUART), BF),
            pltpu.SemaphoreType.DMA,
            pltpu.SemaphoreType.DMA,
        ],
        compiler_params=pltpu.CompilerParams(vmem_limit_bytes=24 * 2**20),
        cost_estimate=pl.CostEstimate(
            flops=10**8, bytes_accessed=2 * 10**6, transcendentals=0
        ),
    )(in_hbm(route_ids.T), in_hbm(expert_in))
    x_got = lax.ppermute(x_give, "sp", other_core)
    x_rows = run(weave_kernel, rows_type, (x_keep, x_got), flops=1e6)
    y_keep, y_give, state_tile, cum, q_dec = run(
        local_kernel,
        (
            side_type, side_type, sds((DK, DV + LANES), BF), sds((TOK, DK), F32),
            sds((TOK, DK), F32),
        ),
        (
            slots, in_hbm(route_weights.T), pick, in_hbm(out_cot), in_hbm(queries), in_hbm(keys),
            in_hbm(values), in_hbm(log_decay),
        ),
        in_specs=[None, None, None, quarter_block(), None, None, None, None],
        flops=3e8,
    )
    y_got = lax.ppermute(y_give, "sp", other_core)
    y_rows = run(weave_kernel, rows_type, (y_keep, y_got), flops=1e6)
    x0 = between_chips(x_rows)
    x0, y_rows = lax.optimization_barrier((x0, y_rows))
    x1 = lax.ppermute(x0, "tp", to_right)
    x2 = lax.ppermute(x0, "tp", to_left)
    xt3 = lax.ppermute(x1[TOP], "tp", to_right)
    xb3 = lax.ppermute(x2[BOTTOM], "tp", to_left)
    y0 = between_chips(y_rows)
    y_top, y_bottom = y0[TOP], y0[BOTTOM]
    t1 = lax.ppermute(y_top, "tp", to_right)
    b2 = lax.ppermute(y_bottom, "tp", to_left)
    b1 = lax.ppermute(y_bottom, "tp", to_right)
    t2 = lax.ppermute(y_top, "tp", to_left)
    t3 = lax.ppermute(t1, "tp", to_right)
    b3 = lax.ppermute(b2, "tp", to_left)
    half_type = sds((SLOTS, FF), F32)
    part_type = sds((SLOTS // 2, QUART), BF)
    g, u = run(gate_near_kernel, (half_type,) * 2, (x0, x1, x2, wg, wu), flops=8e8)
    hidden, to_gate, to_up = run(
        gate_far_kernel,
        (sds((SLOTS, FF), BF), half_type, half_type),
        (g, u, xt3, xb3, wg, wu),
        flops=3e8,
    )
    h = run(near_kernel, half_type, (y0, t1, b1, t2, b2, wd), flops=4e8)
    gate_up, p_top, p_bottom = run(
        far_kernel,
        (sds((SLOTS, 2 * FF), BF), part_type, part_type),
        (h, t3, b3, to_gate, to_up, wg, wu, wd),
        flops=4e8,
    )
    far_top = lax.ppermute(p_top, "tp", to_right)
    far_bottom = lax.ppermute(p_bottom, "tp", to_left)
    p_rt, p_rb, p_lt, p_lb = run(sides_kernel, (part_type,) * 4, (gate_up, wg, wu), flops=5e8)
    bl = lax.ppermute(p_rb, "tp", to_right)
    tr = lax.ppermute(p_lt, "tp", to_left)
    grad_down, p_own = run(
        down_kernel,
        (sds((FF, WIDTH), F32), rows_type),
        (y0, t1, b1, t2, b2, t3, b3, hidden, gate_up, wg, wu),
        flops=8e8,
    )
    far_top, p_own = lax.optimization_barrier((far_top, p_own))
    p_t, p_b = run(merge_kernel, (part_type,) * 2, (p_rt, p_lb, far_top, far_bottom), flops=1e6)
    tl = lax.ppermute(p_t, "tp", to_right)
    br = lax.ppermute(p_b, "tp", to_left)
    grads = run(
        weight_kernel,
        (sds((WIDTH, FF), F32), sds((WIDTH, FF), F32)),
        (x0, x1, x2, xt3, xb3, gate_up),
        flops=1.1e9,
    )
    p_own, grads = lax.optimization_barrier((p_own, grads))
    grad_gate, grad_up = grads
    total = run(sum_kernel, rows_type, (p_own, tl, tr, bl, br), flops=1e6)
    back = between_chips(total)
    give = back.reshape(CHIPS, 2 * CAP, QUART)[:, CAP:, :].reshape(SIDE, QUART)
    got = lax.ppermute(give, "sp", other_core)
    mid = run(
        combine_kernel,
        sds((TOK, QUART), BF),
        (back, got, pick, out_cot),
        in_specs=[None, None, None, quarter_block()],
        flops=7e7,
    )
    m_far = lax.ppermute(mid, "tp", across)
    m_left = lax.ppermute(mid, "tp", to_right)
    m_right = lax.ppermute(mid, "tp", to_left)
    mids = (mid, m_left, m_right, m_far)
    head, pay = run(
        head_kernel,
        (sds((TOK, DV), F32), sds((DK, 2 * DV + LANES), BF)),
        (*mids, w_out, q_dec, state_tile),
        flops=2e8,
    )
    pulled = exchange(pay, in_plane)
    keep, give = run(out_proj_kernel, (sds((1024, DV), BF),) * 2, (*mids, mixed_heads), flops=1.4e8)
    got = lax.ppermute(give, "sp", other_core)
    tiles = run(split_kernel, (tile_type,) * 4, (keep, got), flops=1e6)
    adds = [lax.ppermute(tiles[k], "sp", along_y(k)) for k in (2, 1, 3)]
    state_type = sds((DK, DV), F32)
    pay, suf, pre, factor = run(
        plane_kernel,
        (sds((DK, 4 * DV + LANES), BF), state_type, state_type, state_type),
        (pulled, tiles[0], *adds),
        flops=1e7,
    )
    totals = exchange(pay, along_z)
    pay, grad_out_proj = run(
        line_kernel,
        (sds((DK, 2 * DV), BF), sds((32, DV), F32)),
        (totals, suf, pre, factor),
        flops=1e7,
        scratch=[pltpu.VMEM((DK, DV), F32)],
    )
    back_states = exchange(pay, in_plane)
    d_in = run(
        inside_kernel,
        (sds((TOK, DK), F32), sds((TOK, DK), F32), sds((TOK, DV), F32)),
        (keys, values, cum, q_dec, head),
        flops=3e8,
    )
    grad_queries, grad_keys, grad_values, grad_decay = run(
        last_kernel,
        (
            sds((TOK, DK), BF),
            sds((TOK, DK), BF),
            sds((TOK, DV), BF),
            sds((TOK, DK), F32),
        ),
        (keys, values, cum, q_dec, head, *d_in, back_states),
        flops=3e8,
    )
    return (
        grad_gate[None],
        grad_up[None],
        grad_down[None],
        grad_out_proj,
        grad_queries,
        grad_keys,
        grad_values,
        grad_decay,
    )


def solution(mesh):
    return jax.shard_map(
        per_device,
        mesh=mesh,
        in_specs=(
            P("sp", None),
            P("sp", None),
            P("sp", None),
            P("sp", None),
            P("sp", None, "tp"),
            P("sp", None, "tp"),
            P("sp", "tp", None),
            P(None, "tp"),
            P("sp", "tp"),
            P("sp", "tp"),
            P("sp", "tp"),
            P("sp", "tp"),
            P("sp", "tp"),
        ),
        out_specs=(
            P("sp", None, "tp"),
            P("sp", None, "tp"),
            P("sp", "tp", None),
            P("sp", "tp"),
            P("sp", "tp"),
            P("sp", "tp"),
            P("sp", "tp"),
            P("sp", "tp"),
        ),
        check_vma=False,
    )
```

```python
import functools

import jax
import jax.numpy as jnp
from jax import lax
from jax.experimental import pallas as pl
from jax.experimental.pallas import tpu as pltpu
from jax.sharding import PartitionSpec as P


BF = jnp.bfloat16
F32 = jnp.float32
HI = lax.Precision.HIGHEST

TOK = 128
EXPERTS = 64
CAP = 8
SLOTS = EXPERTS * CAP
SIDE = SLOTS // 2
CHIPS = EXPERTS // 2
WIDTH = 2048
QUART = 512
FF = 256
DK = 128
DV = 256
LANES = 128
HALF = 64


def dot(a, b, ca, cb, precision=None):
    return lax.dot_general(
        a, b, (((ca,), (cb,)), ((), ())), preferred_element_type=F32, precision=precision
    )


def iota(shape, dim):
    return lax.broadcasted_iota(jnp.int32, shape, dim)


def rounded(x):
    return x.astype(BF).astype(F32)


def call(kernel, out_shape, args, *, index, in_specs=None, flops=0, vmem=24, scratch=()):
    nbytes = sum(a.size * a.dtype.itemsize for a in args)
    nbytes += sum(o.size * o.dtype.itemsize for o in jax.tree.leaves(out_shape))

    def whole(a):
        rank = len(a.shape)
        return pl.BlockSpec(a.shape, lambda i, q: (0,) * rank)

    specs = [whole(a) if s is None else s for a, s in zip(args, in_specs or [None] * len(args))]
    return pl.pallas_call(
        kernel,
        out_shape=out_shape,
        grid_spec=pltpu.PrefetchScalarGridSpec(
            num_scalar_prefetch=1,
            grid=(1,),
            in_specs=specs,
            out_specs=jax.tree.map(whole, out_shape),
            scratch_shapes=scratch,
        ),
        compiler_params=pltpu.CompilerParams(vmem_limit_bytes=vmem * 2**20),
        cost_estimate=pl.CostEstimate(
            flops=int(flops), bytes_accessed=int(nbytes), transcendentals=0
        ),
    )(index, *args)


def in_hbm(a):
    return pltpu.with_memory_space_constraint(a, pltpu.HBM)


def sds(shape, dtype):
    return jax.ShapeDtypeStruct(shape, dtype)


def quarter_rows(q):
    return pl.ds(pl.multiple_of(q * QUART, QUART), QUART)


def cumulative_sum(g):
    lower = (iota((TOK, TOK), 0) >= iota((TOK, TOK), 1)).astype(F32)
    return dot(lower, g, 1, 0, HI)


def dot_rounded(a, b, ca, cb):
    high = a.astype(BF)
    return dot(high, b, ca, cb) + dot((a - high.astype(F32)).astype(BF), b, ca, cb)


def pick_kernel(
    ids_hbm, x_ref, keep_ref, give_ref, pick_ref, slot_ref, ids_ref, own_ref, ids_sem, sem
):
    ids_copy = pltpu.make_async_copy(ids_hbm, ids_ref, ids_sem)
    ids_copy.start()
    start = pl.multiple_of(lax.axis_index("tp") * QUART, QUART)
    copy = pltpu.make_async_copy(x_ref.at[:, pl.ds(start, QUART)], own_ref, sem)
    copy.start()
    core = lax.rem(lax.axis_index("sp"), 2)
    expert = iota((EXPERTS, TOK), 0)
    ids_copy.wait()
    id0, id1 = ids_ref[0:1, :], ids_ref[1:2, :]
    hit0, hit1 = expert == id0, expert == id1
    named = (hit0.astype(F32) + hit1.astype(F32)).astype(BF)
    before = (iota((TOK, TOK), 0) < iota((TOK, TOK), 1)).astype(F32).astype(BF)
    count = dot(named, before, 1, 0)
    rank0 = jnp.sum(jnp.where(hit0, count, 0.0), axis=0, keepdims=True)
    rank1 = jnp.sum(jnp.where(hit1, count, 0.0), axis=0, keepdims=True)

    def slot_of(expert_id, rank):
        side = jnp.bitwise_xor(jnp.bitwise_and(expert_id, 1), core)
        return side * SIDE + (expert_id // 2) * CAP + rank.astype(jnp.int32)

    slot0, slot1 = slot_of(id0, rank0), slot_of(id1, rank1)
    slot_ref[0:1, :] = slot0
    slot_ref[1:2, :] = slot1
    slot = iota((SLOTS, TOK), 0)
    pick = ((slot == slot0).astype(F32) + (slot == slot1).astype(F32)).astype(BF)
    pick_ref[...] = pick
    copy.wait()
    rows = dot(pick, own_ref[...], 1, 0).astype(BF)
    keep_ref[...] = rows[:SIDE]
    give_ref[...] = rows[SIDE:]


def weave_kernel(q_ref, keep_ref, got_ref, out_ref):
    keep = keep_ref[...].astype(F32).reshape(CHIPS, CAP, QUART)
    got = got_ref[...].astype(F32).reshape(CHIPS, CAP, QUART)
    out_ref[...] = jnp.concatenate([keep, got], axis=1).reshape(SLOTS, QUART).astype(BF)


def local_kernel(
    q_ref, slot_ref, w_ref, pick_ref, oc_ref, qry_ref, k_ref, v_ref, g_ref,
    keep_ref, give_ref, tile_ref, cum_ref, dec_ref,
):
    slot = iota((SLOTS, TOK), 0)
    at0, at1 = slot == slot_ref[0:1, :], slot == slot_ref[1:2, :]
    weight = jnp.sum(
        jnp.where(at0, w_ref[0:1, :], 0.0) + jnp.where(at1, w_ref[1:2, :], 0.0),
        axis=1,
        keepdims=True,
    )
    rows = (dot(pick_ref[...], oc_ref[...], 1, 0) * weight).astype(BF)
    keep_ref[...] = rows[:SIDE]
    give_ref[...] = rows[SIDE:]
    g = g_ref[...]
    cum = cumulative_sum(g)
    cum_ref[...] = cum
    dec_ref[...] = qry_ref[...].astype(F32) * jnp.exp(cum)
    to_end = k_ref[...].astype(F32) * jnp.exp(cum[TOK - 1 : TOK, :] - cum)
    state = dot(to_end.T, v_ref[...].astype(F32), 1, 0, HI)
    factor = jnp.exp(jnp.sum(g.T, axis=1, keepdims=True))
    high = rounded(factor)
    tile_ref[:, :DV] = state.astype(BF)
    tile_ref[:, DV:] = jnp.where(iota((DK, LANES), 1) < HALF, high, factor - high).astype(BF)


def mark_kernel(q_ref, out_ref):
    out_ref[...] = jnp.full(out_ref.shape, q_ref[0], jnp.int32)


def gate_kernel(
    q_ref, mark_ref, x0_ref, x1_ref, x2_ref, t3_ref, b3_ref, wg_ref, wu_ref,
    hid_ref, to_gate_ref, to_up_ref,
):
    far = jnp.concatenate([t3_ref[...], b3_ref[...]], axis=0)
    g = u = None
    for n, x in enumerate((x0_ref[...], x1_ref[...], x2_ref[...], far)):
        rows = quarter_rows(q_ref[n])
        g1, u1 = dot(x, wg_ref[rows, :], 1, 0), dot(x, wu_ref[rows, :], 1, 0)
        g, u = (g1, u1) if g is None else (g + g1, u + u1)
    sig = jax.nn.sigmoid(g)
    silu = g * sig
    hid_ref[...] = (silu * u).astype(BF)
    to_gate_ref[...] = u * sig * (1.0 + g * (1.0 - sig))
    to_up_ref[...] = silu


TOP, BOTTOM = slice(0, SLOTS // 2), slice(SLOTS // 2, SLOTS)


def near_kernel(q_ref, y0_ref, t1_ref, b1_ref, t2_ref, b2_ref, wd_ref, h_ref):
    w0, w1, w2 = (wd_ref[:, quarter_rows(q_ref[n])] for n in range(3))
    h = dot(y0_ref[...], w0, 1, 1)
    h_ref[TOP, :] = h[TOP] + dot(t1_ref[...], w1, 1, 1) + dot(t2_ref[...], w2, 1, 1)
    h_ref[BOTTOM, :] = h[BOTTOM] + dot(b1_ref[...], w1, 1, 1) + dot(b2_ref[...], w2, 1, 1)


def back_rows(gu_ref, wg_ref, wu_ref, rows):
    part = dot(gu_ref[:, :FF], wg_ref[rows, :], 1, 1) + dot(gu_ref[:, FF:], wu_ref[rows, :], 1, 1)
    return part.astype(BF)


def far_kernel(
    q_ref, h_ref, t3_ref, b3_ref, to_gate_ref, to_up_ref, wg_ref, wu_ref, wd_ref,
    gu_ref, top_ref, bottom_ref,
):
    w3 = wd_ref[:, quarter_rows(q_ref[3])]
    for rows, ref in ((TOP, t3_ref), (BOTTOM, b3_ref)):
        h = h_ref[rows, :] + dot(ref[...], w3, 1, 1)
        gu_ref[rows, :FF] = (h * to_gate_ref[rows, :]).astype(BF)
        gu_ref[rows, FF:] = (h * to_up_ref[rows, :]).astype(BF)
    far = back_rows(gu_ref, wg_ref, wu_ref, quarter_rows(q_ref[3]))
    top_ref[...] = far[TOP]
    bottom_ref[...] = far[BOTTOM]


def sides_kernel(q_ref, gu_ref, wg_ref, wu_ref, rt_ref, rb_ref, lt_ref, lb_ref):
    for n, top_ref, bottom_ref in ((2, rt_ref, rb_ref), (1, lt_ref, lb_ref)):
        part = back_rows(gu_ref, wg_ref, wu_ref, quarter_rows(q_ref[n]))
        top_ref[...] = part[TOP]
        bottom_ref[...] = part[BOTTOM]


def merge_kernel(q_ref, rt_ref, lb_ref, from_left_ref, from_right_ref, t_ref, b_ref):
    t_ref[...] = (rt_ref[...].astype(F32) + from_left_ref[...].astype(F32)).astype(BF)
    b_ref[...] = (lb_ref[...].astype(F32) + from_right_ref[...].astype(F32)).astype(BF)


def down_kernel(
    q_ref, y0_ref, t1_ref, b1_ref, t2_ref, b2_ref, t3_ref, b3_ref, hid_ref, gu_ref, wg_ref, wu_ref,
    gd_ref, own_ref,
):
    own_ref[...] = back_rows(gu_ref, wg_ref, wu_ref, quarter_rows(q_ref[0]))
    hid_t = hid_ref[...].T
    pairs = ((t1_ref, b1_ref), (t2_ref, b2_ref), (t3_ref, b3_ref))
    cots = [y0_ref[...]] + [jnp.concatenate([t[...], b[...]], axis=0) for t, b in pairs]
    for n, dy in enumerate(cots):
        gd_ref[:, quarter_rows(q_ref[n])] = dot(hid_t, dy, 1, 0)


def weight_kernel(
    q_ref, x0_ref, x1_ref, x2_ref, xt_ref, xb_ref, gu_ref, gg_ref, gup_ref
):
    gu = gu_ref[...]
    far = jnp.concatenate([xt_ref[...], xb_ref[...]], axis=0)
    for n, x in enumerate((x0_ref[...], x1_ref[...], x2_ref[...], far)):
        rows = quarter_rows(q_ref[n])
        both = dot(x.T, gu, 1, 0)
        gg_ref[rows, :] = both[:, :FF]
        gup_ref[rows, :] = both[:, FF:]


def sum_kernel(q_ref, own_ref, tl_ref, tr_ref, bl_ref, br_ref, out_ref):
    for rows, a_ref, b_ref in ((TOP, tl_ref, tr_ref), (BOTTOM, bl_ref, br_ref)):
        got = a_ref[...].astype(F32) + b_ref[...].astype(F32)
        out_ref[rows, :] = (own_ref[rows, :].astype(F32) + got).astype(BF)


def combine_kernel(q_ref, rows_ref, got_ref, pick_ref, oc_ref, out_ref):
    keep = rows_ref[...].astype(F32).reshape(CHIPS, 2 * CAP, QUART)[:, :CAP, :]
    keep = keep.reshape(SIDE, QUART).astype(BF)
    pick = pick_ref[...].T
    routed = dot(pick[:, :SIDE], keep, 1, 0) + dot(pick[:, SIDE:], got_ref[...], 1, 0)
    out_ref[...] = (oc_ref[...].astype(F32) + routed).astype(BF)


def head_kernel(
    q_ref, m0_ref, m1_ref, m2_ref, m3_ref, w_ref, dec_ref, tile_ref, h_ref, pay_ref
):
    head = None
    for n, ref in enumerate((m0_ref, m1_ref, m2_ref, m3_ref)):
        part = dot(ref[...], w_ref[quarter_rows(q_ref[n]), :], 1, 0)
        head = part if head is None else head + part
    h_ref[...] = head
    pay_ref[:, :DV] = dot(dec_ref[...].T, head, 1, 0, HI).astype(BF)
    pay_ref[:, DV:] = tile_ref[...]


def out_proj_kernel(q_ref, m0_ref, m1_ref, m2_ref, m3_ref, mixed_ref, keep_ref, give_ref):
    mixed = mixed_ref[...]
    first = q_ref[4] == 0
    for n, ref in enumerate((m0_ref, m1_ref, m2_ref, m3_ref)):
        part = dot(ref[...].T, mixed, 1, 0).reshape(8, 64, DV)
        low = part[:, :32, :].reshape(256, DV)
        high = part[:, 32:, :].reshape(256, DV)
        rows = pl.ds(pl.multiple_of(q_ref[n] * 256, 256), 256)
        keep_ref[rows, :] = jnp.where(first, low, high).astype(BF)
        give_ref[rows, :] = jnp.where(first, high, low).astype(BF)


def split_kernel(q_ref, keep_ref, got_ref, o0_ref, o1_ref, o2_ref, o3_ref):
    total = (keep_ref[...].astype(F32) + got_ref[...].astype(F32)).reshape(8, 128, DV)
    slab = []
    for n in range(4):
        block = total[:, 32 * n : 32 * n + 32, :]
        wide = jnp.concatenate([block[:, :16, :], block[:, 16:, :]], axis=2)
        slab.append(wide.reshape(TOK, 2 * DV))
    y = q_ref[5]
    for k, ref in enumerate((o0_ref, o1_ref, o2_ref, o3_ref)):
        out = slab[k]
        for n in range(1, 4):
            out = jnp.where(y == n, slab[(n + k) % 4], out)
        ref[...] = out.astype(BF)


def block_of(n):
    return slice(16 * n, 16 * n + 16)


def factor_of(ref, lane):
    high, low = ref[:, lane : lane + 1], ref[:, lane + HALF : lane + HALF + 1]
    return jnp.broadcast_to(high.astype(F32) + low.astype(F32), (DK, DV))


def plane_kernel(
    q_ref, in_ref, o_ref, r1_ref, r2_ref, r3_ref, pay_ref, suf_ref, pre_ref, factor_ref
):
    factor_ref[...] = factor_of(in_ref, 2 * DV)
    suf = pre = jnp.zeros((16, DV), F32)
    whole = jnp.ones((16, DV), F32)
    for n in range(8):
        rows = block_of(n)
        pre_ref[rows, :] = pre
        pre = pre * factor_ref[rows, :] + in_ref[rows, DV : 2 * DV].astype(F32)
        whole = whole * factor_ref[rows, :]
        rows = block_of(7 - n)
        suf_ref[rows, :] = suf
        suf = suf * factor_ref[rows, :] + in_ref[rows, :DV].astype(F32)
    part = whole[:, :LANES]
    high = rounded(part)
    part = jnp.where(iota(part.shape, 1) < HALF, high, part - high)
    block = jnp.concatenate([suf, pre, part], axis=1)
    pay_ref[:, : 2 * DV + LANES] = jnp.concatenate([block] * 8, axis=0).astype(BF)
    total = o_ref[...].astype(F32) + r1_ref[...].astype(F32)
    total = total + r2_ref[...].astype(F32) + r3_ref[...].astype(F32)
    pay_ref[:, 2 * DV + LANES :] = total.astype(BF)


def line_kernel(
    q_ref, in_ref, suf_ref, pre_ref, factor_ref, pay_ref, go_ref, totals_ref
):
    totals_ref[...] = factor_of(in_ref, 2 * DV)
    z = q_ref[6]
    suf = pre = jnp.zeros((16, DV), F32)
    for n in range(8):
        rows = block_of(n)
        step = pre * totals_ref[rows, :] + in_ref[rows, DV : 2 * DV].astype(F32)
        pre = jnp.where(n < z, step, pre)
        rows = block_of(7 - n)
        step = suf * totals_ref[rows, :] + in_ref[rows, :DV].astype(F32)
        suf = jnp.where(7 - n > z, step, suf)
    for n in range(8):
        rows = block_of(n)
        pay_ref[rows, DV:] = (pre_ref[rows, :] + pre).astype(BF)
        pre = pre * factor_ref[rows, :]
        rows = block_of(7 - n)
        pay_ref[rows, :DV] = (suf_ref[rows, :] + suf).astype(BF)
        suf = suf * factor_ref[rows, :]
    total = jnp.sum(in_ref[:, 2 * DV + LANES :].astype(F32).reshape(8, 16, 2 * DV), axis=0)
    go_ref[:16, :] = total[:, :DV]
    go_ref[16:, :] = total[:, DV:]


def inside_kernel(
    q_ref, k_ref, v_ref, cum_ref, dec_ref, h_ref, dq_ref, dk_ref, dv_ref
):
    k, v, q_dec, head = k_ref[...].astype(F32), v_ref[...].astype(F32), dec_ref[...], h_ref[...]
    k_grown = k * jnp.exp(-cum_ref[...])
    causal = iota((TOK, TOK), 0) >= iota((TOK, TOK), 1)
    score = jnp.where(causal, dot(q_dec, k_grown, 1, 1, HI), 0.0)
    d_score = jnp.where(causal, dot(head, v, 1, 1, HI), 0.0)
    dq_ref[...] = dot(d_score, k_grown, 1, 0, HI)
    dk_ref[...] = dot(d_score.T, q_dec, 1, 0, HI)
    dv_ref[...] = dot(score.T, head, 1, 0, HI)


def last_kernel(
    q_ref, k_ref, v_ref, cum_ref, dec_ref, h_ref, dq_ref, dk_ref, dv_ref, in_ref,
    gq_ref, gk_ref, gv_ref, gg_ref,
):
    cot, state = in_ref[:, :DV], in_ref[:, DV:]
    k, cum = k_ref[...].astype(F32), cum_ref[...]
    last = cum[TOK - 1 : TOK, :]
    shrink, to_end = jnp.exp(-cum), jnp.exp(last - cum)
    k_end = k * to_end
    d_q = dq_ref[...] + dot_rounded(h_ref[...], state, 1, 1)
    d_kg = dk_ref[...]
    d_ke = dot(v_ref[...], cot, 1, 1)
    gq_ref[...] = (d_q * jnp.exp(cum)).astype(BF)
    gk_ref[...] = (d_kg * shrink + d_ke * to_end).astype(BF)
    gv_ref[...] = (dv_ref[...] + dot_rounded(k_end, cot, 1, 0)).astype(BF)
    end = d_ke * k_end
    d_cum = d_q * dec_ref[...] - d_kg * (k * shrink) - end
    carried = jnp.sum((state.astype(F32) * cot.astype(F32)).T, axis=0, keepdims=True)
    d_last = jnp.sum(end, axis=0, keepdims=True) + jnp.exp(last) * carried
    upper = (iota((TOK, TOK), 0) <= iota((TOK, TOK), 1)).astype(F32)
    gg_ref[...] = dot(upper, d_cum, 1, 0, HI) + d_last


def per_device(
    expert_in, out_cot, route_ids, route_weights, w_gate, w_up, w_down, w_out,
    mixed_heads, queries, keys, values, log_decay,
):
    me, sp = lax.axis_index("tp"), lax.axis_index("sp")
    table = [
        [i, (i + 3) % 4, (i + 1) % 4, (i + 2) % 4, s % 2, s // 2 % 4, s // 8]
        for s in range(64)
        for i in range(4)
    ]
    place = (sp * 4 + me) * 7
    order = lax.dynamic_slice(jnp.array(table, jnp.int32).reshape(-1), (place,), (7,))
    to_right = [(i, (i + 1) % 4) for i in range(4)]
    to_left = [(i, (i + 3) % 4) for i in range(4)]
    across = [(i, (i + 2) % 4) for i in range(4)]
    other_core = [(i, i ^ 1) for i in range(64)]

    def along_y(k):
        return [(i, i // 8 * 8 + (i + 2 * k) % 8) for i in range(64)]

    wg, wu, wd = w_gate[0], w_up[0], w_down[0]
    run = functools.partial(call, index=order)

    def exchange(rows, groups):
        width = rows.shape[1]
        got = lax.all_to_all(
            rows.reshape(8, 16, width), "sp", 0, 0, tiled=True, axis_index_groups=groups
        )
        return got.reshape(DK, width)

    in_plane = [[8 * z + n for n in range(8)] for z in range(8)]
    along_z = [[8 * z + n for z in range(8)] for n in range(8)]

    def quarter_block():
        return pl.BlockSpec((TOK, QUART), lambda i, q: (0, q[0]))

    rows_type = sds((SLOTS, QUART), BF)
    tile_type = sds((TOK, 2 * DV), BF)
    side_type = sds((SIDE, QUART), BF)

    def between_chips(rows):
        groups = [list(range(core, 64, 2)) for core in range(2)]
        got = lax.all_to_all(
            rows.reshape(CHIPS, 2 * CAP, QUART), "sp", 0, 0, tiled=True, axis_index_groups=groups
        )
        return got.reshape(SLOTS, QUART)

    x_keep, x_give, pick, slots = pl.pallas_call(
        pick_kernel,
        out_shape=(side_type, side_type, sds((SLOTS, TOK), BF), sds((2, TOK), jnp.int32)),
        in_specs=[pl.BlockSpec(memory_space=pltpu.HBM)] * 2,
        out_specs=(pl.BlockSpec(memory_space=pltpu.VMEM),) * 4,
        scratch_shapes=[
            pltpu.VMEM((2, TOK), jnp.int32),
            pltpu.VMEM((TOK, QUART), BF),
            pltpu.SemaphoreType.DMA,
            pltpu.SemaphoreType.DMA,
        ],
        compiler_params=pltpu.CompilerParams(vmem_limit_bytes=24 * 2**20),
        cost_estimate=pl.CostEstimate(
            flops=10**8, bytes_accessed=2 * 10**6, transcendentals=0
        ),
    )(in_hbm(route_ids.T), in_hbm(expert_in))
    x_got = lax.ppermute(x_give, "sp", other_core)
    x_rows = run(weave_kernel, rows_type, (x_keep, x_got), flops=1e6)
    y_keep, y_give, state_tile, cum, q_dec = run(
        local_kernel,
        (
            side_type, side_type, sds((DK, DV + LANES), BF), sds((TOK, DK), F32),
            sds((TOK, DK), F32),
        ),
        (
            slots, in_hbm(route_weights.T), pick, in_hbm(out_cot), in_hbm(queries), in_hbm(keys),
            in_hbm(values), in_hbm(log_decay),
        ),
        in_specs=[None, None, None, quarter_block(), None, None, None, None],
        flops=3e8,
    )
    y_got = lax.ppermute(y_give, "sp", other_core)
    y_rows = run(weave_kernel, rows_type, (y_keep, y_got), flops=1e6)
    x0 = between_chips(x_rows)
    x0, y_rows = lax.optimization_barrier((x0, y_rows))
    x1 = lax.ppermute(x0, "tp", to_right)
    x2 = lax.ppermute(x0, "tp", to_left)
    xt3 = lax.ppermute(x1[TOP], "tp", to_right)
    xb3 = lax.ppermute(x2[BOTTOM], "tp", to_left)
    y0 = between_chips(y_rows)
    y_top, y_bottom = y0[TOP], y0[BOTTOM]
    t1 = lax.ppermute(y_top, "tp", to_right)
    b2 = lax.ppermute(y_bottom, "tp", to_left)
    b1 = lax.ppermute(y_bottom, "tp", to_right)
    t2 = lax.ppermute(y_top, "tp", to_left)
    t3 = lax.ppermute(t1, "tp", to_right)
    b3 = lax.ppermute(b2, "tp", to_left)
    half_type = sds((SLOTS, FF), F32)
    part_type = sds((SLOTS // 2, QUART), BF)
    mark = run(mark_kernel, sds((8, LANES), jnp.int32), (), flops=1e4)
    hidden, to_gate, to_up = run(
        gate_kernel,
        (sds((SLOTS, FF), BF), half_type, half_type),
        (mark, x0, x1, x2, xt3, xb3, wg, wu),
        flops=1.1e9,
    )
    h = run(near_kernel, half_type, (y0, t1, b1, t2, b2, wd), flops=4e8)
    gate_up, p_top, p_bottom = run(
        far_kernel,
        (sds((SLOTS, 2 * FF), BF), part_type, part_type),
        (h, t3, b3, to_gate, to_up, wg, wu, wd),
        flops=4e8,
    )
    far_top = lax.ppermute(p_top, "tp", to_right)
    far_bottom = lax.ppermute(p_bottom, "tp", to_left)
    p_rt, p_rb, p_lt, p_lb = run(sides_kernel, (part_type,) * 4, (gate_up, wg, wu), flops=5e8)
    bl = lax.ppermute(p_rb, "tp", to_right)
    tr = lax.ppermute(p_lt, "tp", to_left)
    grad_down, p_own = run(
        down_kernel,
        (sds((FF, WIDTH), F32), rows_type),
        (y0, t1, b1, t2, b2, t3, b3, hidden, gate_up, wg, wu),
        flops=8e8,
    )
    far_top, p_own = lax.optimization_barrier((far_top, p_own))
    p_t, p_b = run(merge_kernel, (part_type,) * 2, (p_rt, p_lb, far_top, far_bottom), flops=1e6)
    tl = lax.ppermute(p_t, "tp", to_right)
    br = lax.ppermute(p_b, "tp", to_left)
    grads = run(
        weight_kernel,
        (sds((WIDTH, FF), F32), sds((WIDTH, FF), F32)),
        (x0, x1, x2, xt3, xb3, gate_up),
        flops=1.1e9,
    )
    p_own, grads = lax.optimization_barrier((p_own, grads))
    grad_gate, grad_up = grads
    total = run(sum_kernel, rows_type, (p_own, tl, tr, bl, br), flops=1e6)
    back = between_chips(total)
    give = back.reshape(CHIPS, 2 * CAP, QUART)[:, CAP:, :].reshape(SIDE, QUART)
    got = lax.ppermute(give, "sp", other_core)
    mid = run(
        combine_kernel,
        sds((TOK, QUART), BF),
        (back, got, pick, out_cot),
        in_specs=[None, None, None, quarter_block()],
        flops=7e7,
    )
    m_far = lax.ppermute(mid, "tp", across)
    m_left = lax.ppermute(mid, "tp", to_right)
    m_right = lax.ppermute(mid, "tp", to_left)
    mids = (mid, m_left, m_right, m_far)
    head, pay = run(
        head_kernel,
        (sds((TOK, DV), F32), sds((DK, 2 * DV + LANES), BF)),
        (*mids, w_out, q_dec, state_tile),
        flops=2e8,
    )
    pulled = exchange(pay, in_plane)
    keep, give = run(out_proj_kernel, (sds((1024, DV), BF),) * 2, (*mids, mixed_heads), flops=1.4e8)
    got = lax.ppermute(give, "sp", other_core)
    tiles = run(split_kernel, (tile_type,) * 4, (keep, got), flops=1e6)
    adds = [lax.ppermute(tiles[k], "sp", along_y(k)) for k in (2, 1, 3)]
    state_type = sds((DK, DV), F32)
    pay, suf, pre, factor = run(
        plane_kernel,
        (sds((DK, 4 * DV + LANES), BF), state_type, state_type, state_type),
        (pulled, tiles[0], *adds),
        flops=1e7,
    )
    totals = exchange(pay, along_z)
    pay, grad_out_proj = run(
        line_kernel,
        (sds((DK, 2 * DV), BF), sds((32, DV), F32)),
        (totals, suf, pre, factor),
        flops=1e7,
        scratch=[pltpu.VMEM((DK, DV), F32)],
    )
    back_states = exchange(pay, in_plane)
    d_in = run(
        inside_kernel,
        (sds((TOK, DK), F32), sds((TOK, DK), F32), sds((TOK, DV), F32)),
        (keys, values, cum, q_dec, head),
        flops=3e8,
    )
    grad_queries, grad_keys, grad_values, grad_decay = run(
        last_kernel,
        (
            sds((TOK, DK), BF),
            sds((TOK, DK), BF),
            sds((TOK, DV), BF),
            sds((TOK, DK), F32),
        ),
        (keys, values, cum, q_dec, head, *d_in, back_states),
        flops=3e8,
    )
    return (
        grad_gate[None],
        grad_up[None],
        grad_down[None],
        grad_out_proj,
        grad_queries,
        grad_keys,
        grad_values,
        grad_decay,
    )


def solution(mesh):
    return jax.shard_map(
        per_device,
        mesh=mesh,
        in_specs=(
            P("sp", None),
            P("sp", None),
            P("sp", None),
            P("sp", None),
            P("sp", None, "tp"),
            P("sp", None, "tp"),
            P("sp", "tp", None),
            P(None, "tp"),
            P("sp", "tp"),
            P("sp", "tp"),
            P("sp", "tp"),
            P("sp", "tp"),
            P("sp", "tp"),
        ),
        out_specs=(
            P("sp", None, "tp"),
            P("sp", None, "tp"),
            P("sp", "tp", None),
            P("sp", "tp"),
            P("sp", "tp"),
            P("sp", "tp"),
            P("sp", "tp"),
            P("sp", "tp"),
        ),
        check_vma=False,
    )
```
